256 devices in a mesh: rep: 32 (over z, y), fs: 4 (over x), tp: 2 (over core).
Axes of the slice: x: 4, y: 4, z: 8, core: 2. Of those that a mesh axis runs over, the one named last changes fastest.
Arguments:
- tokens: bfloat16 [32768, 2048], P(('rep', 'fs', 'tp')), may hold values from -24 to 24
- cotangent: bfloat16 [32768, 2048], P(('rep', 'fs', 'tp')), may hold values from -24 to 24
- gate_weight: bfloat16 [2048, 3072], P(None, 'fs'), may hold values from -0.125 to 0.125
- up_weight: bfloat16 [2048, 3072], P(None, 'fs'), may hold values from -0.125 to 0.125
- down_weight_t: bfloat16 [2048, 3072], P(None, 'fs'), may hold values from -0.109375 to 0.109375
Outputs:
- input_grad: bfloat16 [32768, 2048], P(('rep', 'fs', 'tp'))
- gate_grad: float32 [2048, 3072], P(('rep', 'tp'), 'fs')
- up_grad: float32 [2048, 3072], P(('rep', 'tp'), 'fs')
- down_grad: float32 [2048, 3072], P(('rep', 'tp'), 'fs')
The draws below stay inside these ranges and needn't reach their ends.
All inputs are finite; a program needn't handle non-finite values.
Results may differ from the reference program's by a relative error of at most 0.012.
Values may be sent and summed in bfloat16 or wider, within the bound.
A program may use at most 128 MiB of HBM per device.

```python
import jax
import jax.numpy as jnp
from jax import lax

D = 2048
FF = 3072
TOKENS = 32768
N_REP = 32
N_FS = 4


def raised(result, rng, source, target, blocks, factor):
    def block_of(axis_at):
        return (jnp.arange(result.shape[axis_at]) // (result.shape[axis_at] // blocks)).reshape((-1,) + (1,) * (result.ndim - 1 - axis_at))

    first = jax.random.permutation(rng, blocks)[block_of(target)]
    other_side = (block_of(target) + blocks // 2) % blocks
    return jnp.where((block_of(source) == first) | (block_of(source) == other_side), factor * result, result)


def block_levels(rng, shape, shards, low, top_value):
    def one(dim, shards_of):
        heights = jax.random.uniform(jax.random.fold_in(jax.random.fold_in(rng, 6), dim), (shards_of,), jnp.float32, low / len(shards), top_value / len(shards))
        return jnp.repeat(jnp.exp(heights), shape[dim] // shards_of).reshape((-1,) + (1,) * (len(shape) - dim - 1))

    loudness = one(*shards[0])
    for cut in shards[1:]:
        loudness = loudness * one(*cut)
    return loudness


def gaussian(key, extent, width, limit, split=(), kind=jnp.bfloat16):
    loudness = block_levels(key, extent, split, -0.22, 0.18) if split else 1.0
    result = jax.random.normal(key, extent, jnp.float32) * width * loudness
    return jnp.minimum(jnp.maximum(result, -limit), limit).astype(kind)


def noise_with(key, dims, width, most, pieces, heavy, held_as=jnp.bfloat16):
    values = width * jax.random.normal(key, dims, jnp.float32)
    if pieces:
        values = values * block_levels(key, dims, pieces, -0.22, 0.18)
    return jnp.clip(raised(values, jax.random.fold_in(key, 3), *heavy), -most, most).astype(held_as)


def setup_inputs(seed: int = 0) -> dict:
    arg_keys = jax.random.split(jax.random.key(seed), 6)
    tokens = noise_with(arg_keys[0], (TOKENS, D), 1.0, 24.0, ((0, 256),), (0, 1, 256, 6.0))
    cotangent = noise_with(arg_keys[1], (TOKENS, D), 1.0, 24.0, ((0, 256),), (0, 1, 256, 6.0))
    gate_weight = gaussian(arg_keys[2], (D, FF), D ** -0.5, 0.125, ((1, 4),))
    up_weight = gaussian(arg_keys[3], (D, FF), D ** -0.5, 0.125, ((1, 4),))
    down_weight_t = gaussian(arg_keys[4], (D, FF), FF ** -0.5, 0.109375, ((1, 4),))
    return dict(tokens=tokens, cotangent=cotangent, gate_weight=gate_weight, up_weight=up_weight, down_weight_t=down_weight_t)


def reference(tokens, cotangent, gate_weight, up_weight, down_weight_t):
    row_block = TOKENS // N_REP
    hid_width = FF // N_FS
    gate_split = gate_weight.astype(jnp.float32).reshape(D, N_FS, hid_width)
    up_split = up_weight.astype(jnp.float32).reshape(D, N_FS, hid_width)

    def accumulate(totals, block_index):
        first_row = block_index * row_block
        tok_rows = lax.dynamic_slice_in_dim(tokens, first_row, row_block, 0)
        cot_rows = lax.dynamic_slice_in_dim(cotangent, first_row, row_block, 0)
        gate_pre = jnp.dot(tok_rows, gate_weight, preferred_element_type=jnp.float32)
        up_pre = jnp.dot(tok_rows, up_weight, preferred_element_type=jnp.float32)
        sig_gate = jax.nn.sigmoid(gate_pre)
        act_gate = gate_pre * sig_gate
        hidden = (act_gate * up_pre).astype(jnp.bfloat16)
        hid_grad = jnp.dot(cot_rows, down_weight_t, preferred_element_type=jnp.float32)
        gate_back = (hid_grad * up_pre * sig_gate * (1.0 + gate_pre * (1.0 - sig_gate))).astype(jnp.bfloat16)
        up_back = (hid_grad * act_gate).astype(jnp.bfloat16)
        partial_value = jnp.einsum("rnf,dnf->nrd", gate_back.astype(jnp.float32).reshape(row_block, N_FS, hid_width),
                             gate_split, precision=lax.Precision.HIGHEST)
        partial_value = partial_value + jnp.einsum("rnf,dnf->nrd", up_back.astype(jnp.float32).reshape(row_block, N_FS, hid_width),
                                       up_split, precision=lax.Precision.HIGHEST)
        rounded = lax.optimization_barrier(partial_value.astype(jnp.bfloat16))
        input_rows = jnp.sum(rounded.astype(jnp.float32), axis=0).astype(jnp.bfloat16)
        new_totals = (totals[0] + jnp.dot(tok_rows.T, gate_back, preferred_element_type=jnp.float32),
                      totals[1] + jnp.dot(tok_rows.T, up_back, preferred_element_type=jnp.float32),
                      totals[2] + jnp.dot(cot_rows.T, hidden, preferred_element_type=jnp.float32))
        return new_totals, input_rows

    zeros = jnp.zeros((D, FF), jnp.float32)
    totals, input_blocks = lax.scan(accumulate, (zeros, zeros, zeros), jnp.arange(N_REP, dtype=jnp.int32))
    grad_scale = float(TOKENS) ** -0.5
    return (input_blocks.reshape(TOKENS, D), totals[0] * grad_scale, totals[1] * grad_scale, totals[2] * grad_scale)
```

```python
import jax
import jax.numpy as jnp
from jax import lax
from jax.sharding import PartitionSpec as P


def joined_along(parts, dim):
    parts = jnp.moveaxis(parts, 0, dim)
    shape = parts.shape
    return parts.reshape(*shape[:dim], shape[dim] * shape[dim + 1], *shape[dim + 2 :])


def copy_for_each(value, axis):
    copies = jnp.broadcast_to(value, (lax.axis_size(axis), *value.shape))
    return lax.all_to_all(copies, axis, split_axis=0, concat_axis=0, tiled=True)


def gathered_copies(value, axis, dim):
    return joined_along(copy_for_each(value, axis), dim)


def in_one_piece(arrays, axis, dim, along):
    widths = [a.shape[along] for a in arrays]
    both = jnp.concatenate(arrays, axis=along)
    whole = lax.all_gather(both, axis, axis=dim, tiled=True)
    return tuple(jnp.split(whole, [sum(widths[:k]) for k in range(1, len(widths))], axis=along))


def in_blocks(value, dim, peers):
    before, after = (value.shape[:dim], value.shape[dim + 1 :])
    return jnp.moveaxis(value.reshape(*before, peers, -1, *after), dim, 0)


def sum_at_owner(value, axis, dim):
    parts = in_blocks(value, dim, lax.axis_size(axis))
    arrived = lax.all_to_all(parts, axis, split_axis=0, concat_axis=0, tiled=True)
    return arrived.astype(jnp.float32).sum(axis=0)


def in_one_piece_2(arrays, axis, dim, along):
    both = jnp.concatenate([a.astype(jnp.bfloat16) for a in arrays], axis=along)
    whole, at, finished = (lax.psum_scatter(both, axis, scatter_dimension=dim, tiled=True), 0, [])
    for a in arrays:
        finished.append(
            lax.slice_in_dim(whole, at, at + a.shape[along], axis=along).astype(jnp.float32)
        )
        at += a.shape[along]
    return tuple(finished)


def on_device(tokens, cotangent, gate_weight, up_weight, down_weight_t):
    tok_rows, cot_rows = in_one_piece((tokens, cotangent), "fs", 0, 1)
    gate_pre = jnp.dot(tok_rows, gate_weight, preferred_element_type=jnp.float32)
    up_pre = jnp.dot(tok_rows, up_weight, preferred_element_type=jnp.float32)
    sig_gate = jax.nn.sigmoid(gate_pre)
    act_gate = gate_pre * sig_gate
    hidden = (act_gate * up_pre).astype(jnp.bfloat16)
    hid_grad = jnp.dot(cot_rows, down_weight_t, preferred_element_type=jnp.float32)
    local_gate_back = (hid_grad * up_pre * sig_gate * (1.0 + gate_pre * (1.0 - sig_gate))).astype(
        jnp.bfloat16
    )
    local_up_back = (hid_grad * act_gate).astype(jnp.bfloat16)
    tok_all, cot_all, gate_back, up_back, hidden = (
        tok_rows,
        cot_rows,
        local_gate_back,
        local_up_back,
        hidden,
    )
    own_rows = tokens.shape[0]
    across = (((1,), (1,)), ((), ()))
    input_grad = sum_at_owner(
        (
            lax.dot_general(gate_back, gate_weight, across, preferred_element_type=jnp.float32)
            + lax.dot_general(up_back, up_weight, across, preferred_element_type=jnp.float32)
        ).astype(jnp.bfloat16),
        "fs",
        0,
    ).astype(jnp.bfloat16)
    replicas = lax.axis_size("rep")
    cores = lax.axis_size("tp")
    shards = lax.axis_size("fs")
    grad_scale = float(own_rows * replicas * shards * cores) ** (-0.5)
    down_rows = (((0,), (0,)), ((), ()))
    gate_local = (
        lax.dot_general(tok_all, gate_back, down_rows, preferred_element_type=jnp.float32)
        * grad_scale
    )
    up_local = (
        lax.dot_general(tok_all, up_back, down_rows, preferred_element_type=jnp.float32)
        * grad_scale
    )
    down_local = (
        lax.dot_general(cot_all, hidden, down_rows, preferred_element_type=jnp.float32) * grad_scale
    )
    summed = in_one_piece_2((gate_local, up_local, down_local), ("rep", "tp"), 0, 1)
    return (input_grad, summed[0], summed[1], summed[2])


def solution(mesh):
    return jax.shard_map(
        on_device,
        mesh=mesh,
        in_specs=(
            P(("rep", "fs", "tp"), None),
            P(("rep", "fs", "tp"), None),
            P(None, "fs"),
            P(None, "fs"),
            P(None, "fs"),
        ),
        out_specs=(
            P(("rep", "fs", "tp"), None),
            P(("rep", "tp"), "fs"),
            P(("rep", "tp"), "fs"),
            P(("rep", "tp"), "fs"),
        ),
        check_vma=False,
    )
```

```python
import functools
import heapq

import jax
import jax.numpy as jnp
from jax import lax
from jax.experimental import pallas as pl
from jax.experimental.pallas import tpu as pltpu
from jax.sharding import PartitionSpec as P

MESH = pl.DeviceIdType.MESH
F32 = jnp.float32
BF16 = jnp.bfloat16

NY, NZ = 4, 8
BLOCKS = ((0, 256, "z"), (256, 256, "y"), (512, 256, "z"), (768, 256, "y"), (1024, 128, "z"))


def chains_of(n):
    return ((1, 0, n // 2), (-1, 1, n // 2), (1, 1, n // 2 - 1), (-1, 0, n // 2 - 1))


class Ring:
    def __init__(self, block, phase, axis, first_slot):
        self.block, self.phase, self.axis = block, phase, axis
        self.n = NY if axis == "y" else NZ
        self.chains = chains_of(self.n)
        self.slots, at = {}, 0
        for c, (_, _, start) in enumerate(self.chains):
            for d in range(start, 0, -1):
                self.slots[c, d] = at
                at += 1
        self.count, self.first_slot = at, first_slot

    def half_shape(self):
        width = BLOCKS[self.block][1]
        if self.phase == 2:
            return (32, width)
        return (NZ // 2, 64, width) if self.axis == "y" else (NY // 2, 64, width)

    def half_bytes(self):
        size = 2
        for extent in self.half_shape():
            size *= extent
        return size


def all_rings():
    rings, slot = {}, 0
    for b, (_, _, first) in enumerate(BLOCKS):
        for phase, axis in ((1, first), (2, "z" if first == "y" else "y")):
            rings[b, phase] = Ring(b, phase, axis, slot)
            slot += rings[b, phase].count
    return rings, slot


def schedule(rings, rate=46.0e3, latency=2.7, step=0.2):
    free, arrivals, order, left, tick = {}, [], [], {}, [0]

    def send(key, c, d, now):
        ring = rings[key]
        link = (ring.axis, ring.chains[c][0])
        free[link] = max(free.get(link, 0.0), now) + ring.half_bytes() / rate
        tick[0] += 1
        heapq.heappush(arrivals, (free[link] + latency, tick[0], key, c, d))

    def begin(key, now):
        left[key] = 4
        for c, (_, _, start) in enumerate(rings[key].chains):
            send(key, c, start, now)

    for b in range(len(BLOCKS)):
        begin((b, 1), 0.0)
    now = 0.0
    while arrivals:
        at, _, key, c, d = heapq.heappop(arrivals)
        now = max(now, at) + step
        order.append((key, c, d))
        if d > 1:
            send(key, c, d - 1, now)
        else:
            left[key] -= 1
            if left[key] == 0 and key[1] == 1:
                begin((key[0], 2), now)
    return order, now


def kernel(tok_hbm, cot_hbm, wg_hbm, wu_hbm, wd_hbm,
           ig_out, gate_out, up_out, down_out,
           xb, wgu, wd, gub, hid, acc, own_ig, ig_part, ig_send0, ig_send, ig_recv0, ig_recv,
           xr1, xr2, *rest):
    nb = len(BLOCKS)
    blks, rest = rest[:nb], rest[nb:]
    rings, total_slots = all_rings()
    keys = [(b, phase) for b in range(nb) for phase in (1, 2)]
    rbufs, rest = dict(zip(keys, rest[: 2 * nb])), rest[2 * nb :]
    fins, rest = rest[:nb], rest[nb:]
    finr, rest = rest[:nb], rest[nb:]
    (load_sem, ag_send, ag_recv, rel_send, rel_recv, igx_send, igx_recv,
     xrs_send, xrs_recv, ring_send, ring_recv, fin_send, fin_recv) = rest

    rep, x, core = lax.axis_index("rep"), lax.axis_index("fs"), lax.axis_index("tp")
    z, y = rep // NY, lax.rem(rep, NY)
    right = (rep, lax.rem(x + 1, 4), core)
    left = (rep, lax.rem(x + 3, 4), core)
    partner = (rep, x, 1 - core)
    y_of = {s: (z * NY + lax.rem(y + s + NY, NY), x, core) for s in (1, -1)}
    z_of = {s: (lax.rem(z + s + NZ, NZ) * NY + y, x, core) for s in (1, -1)}

    def remote(src, dst, send_sem, recv_sem, to):
        return pltpu.make_async_remote_copy(src_ref=src, dst_ref=dst, send_sem=send_sem,
                                            recv_sem=recv_sem, device_id=to, device_id_type=MESH)

    cols = pl.ds(pl.multiple_of(core * 384, 128), 384)
    load_tok = pltpu.make_async_copy(tok_hbm, xb.at[0, 0], load_sem.at[0])
    load_cot = pltpu.make_async_copy(cot_hbm, xb.at[0, 1], load_sem.at[1])
    load_w = [
        pltpu.make_async_copy(wg_hbm.at[:, cols], wgu.at[:, pl.ds(0, 384)], load_sem.at[2]),
        pltpu.make_async_copy(wu_hbm.at[:, cols], wgu.at[:, pl.ds(384, 384)], load_sem.at[3]),
        pltpu.make_async_copy(wd_hbm.at[:, cols], wd, load_sem.at[4]),
    ]
    load_tok.start()
    load_cot.start()
    for copy in load_w:
        copy.start()

    barrier = pltpu.get_barrier_semaphore()
    for other in (right, left, partner, y_of[1], y_of[-1], z_of[1], z_of[-1]):
        pl.semaphore_signal(barrier, inc=1, device_id=other, device_id_type=MESH)
    pl.semaphore_wait(barrier, 7)
    load_tok.wait()
    load_cot.wait()

    def own_piece(k, side):
        piece = k if side == 0 else (k + 2) % 4
        return remote(xb.at[0, :, pl.ds(32 * piece, 32)], xb.at[2 + k, :, pl.ds(32 * side, 32)],
                      ag_send.at[side, k], ag_recv.at[side, k], right if side == 0 else left)

    def passed_on(k, side):
        return remote(xb.at[2 + k, :, pl.ds(32 * side, 32)], xb.at[6 + k, :, pl.ds(32 * side, 32)],
                      ag_send.at[side, 4 + k], ag_recv.at[side, 4 + k], right if side == 0 else left)

    def arrival(k, side):
        here = xb.at[2 + k, :, pl.ds(32 * side, 32)]
        return remote(here, here, ag_send.at[side, k], ag_recv.at[side, k],
                      right if side == 0 else left)

    def relay(k):
        return remote(xb.at[2 + k, :, pl.ds(0, 64)], xb.at[2 + k, :, pl.ds(64, 64)],
                      rel_send.at[k], rel_recv.at[k], partner)

    own_to_partner = remote(xb.at[0], xb.at[1], rel_send.at[6], rel_recv.at[6], partner)
    for k in range(4):
        for side in (0, 1):
            own_piece(k, side).start()
        if k == 0:
            own_to_partner.start()
    for copy in load_w:
        copy.wait()

    def forward(s):
        rows = pl.ds(pl.multiple_of(s * 128, 128), 128)
        gu = jnp.dot(xb[s, 0], wgu[...], preferred_element_type=F32)
        hg = jnp.dot(xb[s, 1], wd[...], preferred_element_type=F32)
        gate, up = gu[:, :384], gu[:, 384:]
        sig = jax.nn.sigmoid(gate)
        act = gate * sig
        gub[rows, pl.ds(0, 384)] = (hg * up * sig * (1.0 + gate * (1.0 - sig))).astype(BF16)
        gub[rows, pl.ds(384, 384)] = (hg * act).astype(BF16)
        hid[rows, :] = (act * up).astype(BF16)

    def input_part(s, store):
        rows = pl.ds(pl.multiple_of(s * 128, 128), 128)

        def some(n, carry):
            d = pl.ds(pl.multiple_of(n * 512, 512), 512)
            part = lax.dot_general(gub[rows, :], wgu[d, :], (((1,), (1,)), ((), ())),
                                   preferred_element_type=F32)
            store(d, part.astype(BF16))
            return carry

        lax.fori_loop(0, 4, some, 0)

    def store_own(d, part):
        own_ig[:, d] = part

    def store_partner(d, part):
        ig_send0[:, d] = part

    send_ig0 = remote(ig_send0, ig_recv0, igx_send.at[6], igx_recv.at[6], partner)

    def send_ig(k):
        return remote(ig_send.at[k], ig_recv.at[k], igx_send.at[k], igx_recv.at[k], partner)

    def step_part(s):
        k = s - 2

        def store(d, part):
            ig_part[k, :, d] = part[:64]
            ig_send[k, :, d] = part[64:]

        input_part(s, store)
        send_ig(k).start()

    forward(0)
    input_part(0, store_own)
    own_to_partner.wait_recv()
    forward(1)
    input_part(1, store_partner)
    send_ig0.start()

    def take(k):
        arrival(k, 0).wait_recv()
        arrival(k, 1).wait_recv()
        relay(k).start()

    def early(k, carry):
        take(k)

        @pl.when(k < 2)
        def _():
            passed_on(k, 0).start()
            passed_on(k, 1).start()

        relay(k).wait_recv()
        forward(k + 2)
        step_part(k + 2)
        return carry

    lax.fori_loop(0, 4, early, 0)

    across = (((0,), (0,)), ((), ()))

    def products(j, first, count):
        d = pl.ds(pl.multiple_of(j * 256, 256), 256)
        rows = pl.ds(first * 128, count * 128)
        tok = xb[pl.ds(first, count), 0, :, d].reshape(count * 128, 256)
        cot = xb[pl.ds(first, count), 1, :, d].reshape(count * 128, 256)
        return (lax.dot_general(tok, gub[rows, :], across, preferred_element_type=F32),
                lax.dot_general(cot, hid[rows, :], across, preferred_element_type=F32))

    def first_sums(j, carry):
        a, b = products(j, 0, 6)
        acc[j, :, pl.ds(0, 768)] = a
        acc[j, :, pl.ds(768, 384)] = b
        return carry

    lax.fori_loop(0, 8, first_sums, 0)

    take(4)
    relay(4).wait_recv()
    forward(6)
    step_part(6)
    take(5)
    relay(5).wait_recv()
    forward(7)

    def last_sums(j, carry):
        a, b = products(j, 6, 2)
        a = (acc[j, :, pl.ds(0, 768)] + a).astype(BF16)
        b = (acc[j, :, pl.ds(768, 384)] + b).astype(BF16)
        for i, (col, width, _) in enumerate(BLOCKS):
            piece = a[:, col : col + width] if col < 768 else b[:, col - 768 : col - 768 + width]
            blks[i][j] = piece.reshape(NY, 64, width)
        return carry

    lax.fori_loop(0, 8, last_sums, 0)

    def half_of(ring, j, half):
        blk = blks[ring.block]
        if ring.phase == 1:
            if ring.axis == "y":
                return blk.at[pl.ds(4 * half, 4), j]
            return blk.at[j, pl.ds(2 * half, 2)]
        if ring.axis == "z":
            return blk.at[j, y, pl.ds(32 * half, 32)]
        return blk.at[z, j, pl.ds(32 * half, 32)]

    def place(ring, offset):
        if ring.axis == "y":
            return lax.rem(y + offset + NY, NY)
        return lax.rem(z + offset + NZ, NZ)

    def hop(key, c, d):
        ring = rings[key]
        sign, half, _ = ring.chains[c]
        slot = ring.slots[c, d]
        sem = ring.first_slot + slot
        return remote(half_of(ring, place(ring, sign * d), half), rbufs[key].at[slot],
                      ring_send.at[sem], ring_recv.at[sem],
                      (y_of if ring.axis == "y" else z_of)[sign])

    def begin(key):
        for c, (_, _, start) in enumerate(rings[key].chains):
            hop(key, c, start).start()

    def add_into(dst, src):
        shape = dst.shape
        if len(shape) == 2:
            dst[...] = (dst[...].astype(F32) + src[...].astype(F32)).astype(BF16)
        else:
            def one(i, carry):
                dst[i] = (dst[i].astype(F32) + src[i].astype(F32)).astype(BF16)
                return carry
            lax.fori_loop(0, shape[0], one, 0)

    for b in range(nb):
        begin((b, 1))

    step_part(7)

    def xrs(stage, way):
        rows = pl.ds(32 * way, 32)
        which = {0: (4, 2), 1: (2, 2), 2: (0, 2)}[stage]
        dst = xr1.at[way] if stage == 0 else xr2.at[way, pl.ds(which[0], 2)]
        return remote(ig_part.at[pl.ds(which[0], 2), rows], dst, xrs_send.at[stage, way],
                      xrs_recv.at[stage, way], left if way == 0 else right)

    def merge_part(k, carry):
        send_ig(k).wait_recv()
        ig_part[k] = (ig_part[k].astype(F32) + ig_recv[k].astype(F32)).astype(BF16)
        return carry

    lax.fori_loop(2, 6, merge_part, 0)
    for stage in (0, 1):
        for way in (0, 1):
            xrs(stage, way).start()
    lax.fori_loop(0, 2, merge_part, 0)
    send_ig0.wait_recv()

    def x_middle():
        for way in (0, 1):
            xrs(0, way).wait_recv()
        for k in range(2):
            for way in (0, 1):
                rows = pl.ds(32 * way, 32)
                ig_part[k, rows, :] = (ig_part[k, rows, :].astype(F32)
                                       + xr1[way, k].astype(F32)).astype(BF16)
        for way in (0, 1):
            xrs(2, way).start()

    def x_end():
        for stage in (1, 2):
            for way in (0, 1):
                xrs(stage, way).wait_recv()
        for piece in range(4):
            rows = pl.ds(32 * piece, 32)
            total = own_ig[rows, :].astype(F32) + ig_recv0[rows, :].astype(F32)
            total = total + xr2[0, piece].astype(F32) + xr2[1, (piece + 2) % 4].astype(F32)
            ig_out[rows, :] = total.astype(BF16)

    order, _ = schedule(rings)
    left_of = {key: 4 for key in keys}
    scale = float(32768) ** -0.5

    def fin_copy(b):
        return remote(fins[b].at[pl.ds(pl.multiple_of((1 - core) * 32, 32), 32)], finr[b],
                      fin_send.at[b], fin_recv.at[b], partner)

    def finish_block(b):
        ring = rings[b, 2]
        for half in (0, 1):
            total = half_of(rings[b, 2], place(ring, 0), half)[...].astype(F32)
            for c, (_, h, _) in enumerate(ring.chains):
                if h == half:
                    total = total + rbufs[b, 2][ring.slots[c, 1]].astype(F32)
            fins[b][pl.ds(32 * half, 32), :] = total * scale
        fin_copy(b).start()

    for at, (key, c, d) in enumerate(order):
        ring = rings[key]
        sign, half, _ = ring.chains[c]
        hop(key, c, d).wait_recv()
        if d > 1:
            add_into(half_of(ring, place(ring, sign * (d - 1)), half), rbufs[key].at[ring.slots[c, d]])
            hop(key, c, d - 1).start()
        else:
            left_of[key] -= 1
            if key[1] == 1:
                add_into(half_of(ring, place(ring, 0), half), rbufs[key].at[ring.slots[c, d]])
                if left_of[key] == 0:
                    begin((key[0], 2))
            elif left_of[key] == 0:
                finish_block(key[0])
        if at == 3 * len(order) // 10:
            x_middle()
        if at == 7 * len(order) // 10:
            x_end()

    def place_out(b, value, which):
        col, width, _ = BLOCKS[b]
        at = col
        while at < col + width:
            take_n = min(384 - at % 384, col + width - at)
            out = (gate_out, up_out, down_out)[at // 384]
            out[:, pl.ds(pl.multiple_of(which * 384 + at % 384, 128), take_n)] = (
                value[:, at - col : at - col + take_n])
            at += take_n

    mine = pl.ds(pl.multiple_of(core * 32, 32), 32)
    for b in range(nb):
        place_out(b, fins[b][mine, :], core)
    for b in range(nb):
        fin_copy(b).wait_recv()
        place_out(b, finr[b][...], 1 - core)

    for k in range(4):
        for side in (0, 1):
            own_piece(k, side).wait_send()
    for k in range(2):
        for side in (0, 1):
            passed_on(k, side).wait_send()
    for k in range(6):
        relay(k).wait_send()
        send_ig(k).wait_send()
    own_to_partner.wait_send()
    send_ig0.wait_send()
    for stage in range(3):
        for way in (0, 1):
            xrs(stage, way).wait_send()
    for key, c, d in order:
        hop(key, c, d).wait_send()
    for b in range(nb):
        fin_copy(b).wait_send()


def on_device(tokens, cotangent, gate_weight, up_weight, down_weight_t):
    rings, slots = all_rings()
    keys = [(b, phase) for b in range(len(BLOCKS)) for phase in (1, 2)]
    anywhere = pl.BlockSpec(memory_space=pl.ANY)
    vmem = pl.BlockSpec(memory_space=pltpu.VMEM)
    dma = pltpu.SemaphoreType.DMA
    return pl.pallas_call(
        kernel,
        out_shape=(
            jax.ShapeDtypeStruct((128, 2048), BF16),
            jax.ShapeDtypeStruct((32, 768), F32),
            jax.ShapeDtypeStruct((32, 768), F32),
            jax.ShapeDtypeStruct((32, 768), F32),
        ),
        in_specs=[anywhere] * 5,
        out_specs=[vmem] * 4,
        scratch_shapes=[
            pltpu.VMEM((8, 2, 128, 2048), BF16),
            pltpu.VMEM((2048, 768), BF16),
            pltpu.VMEM((2048, 384), BF16),
            pltpu.VMEM((1024, 768), BF16),
            pltpu.VMEM((1024, 384), BF16),
            pltpu.VMEM((8, 256, 1152), F32),
            pltpu.VMEM((128, 2048), BF16),
            pltpu.VMEM((6, 64, 2048), BF16),
            pltpu.VMEM((128, 2048), BF16),
            pltpu.VMEM((6, 64, 2048), BF16),
            pltpu.VMEM((128, 2048), BF16),
            pltpu.VMEM((6, 64, 2048), BF16),
            pltpu.VMEM((2, 2, 32, 2048), BF16),
            pltpu.VMEM((2, 4, 32, 2048), BF16),
        ]
        + [pltpu.VMEM((NZ, NY, 64, width), BF16) for _, width, _ in BLOCKS]
        + [pltpu.VMEM((rings[key].count, *rings[key].half_shape()), BF16) for key in keys]
        + [pltpu.VMEM((64, width), F32) for _, width, _ in BLOCKS]
        + [pltpu.VMEM((32, width), F32) for _, width, _ in BLOCKS]
        + [
            dma((5,)), dma((2, 6)), dma((2, 6)), dma((7,)), dma((7,)), dma((7,)), dma((7,)),
            dma((3, 2)), dma((3, 2)), dma((slots,)), dma((slots,)),
            dma((len(BLOCKS),)), dma((len(BLOCKS),)),
        ],
        compiler_params=pltpu.CompilerParams(
            collective_id=0, has_side_effects=True, vmem_limit_bytes=62 * 1024 * 1024
        ),
    )(tokens, cotangent, gate_weight, up_weight, down_weight_t)


def solution(mesh):
    rows, tall = P(("rep", "fs", "tp"), None), P(("rep", "tp"), "fs")
    return jax.shard_map(
        on_device,
        mesh=mesh,
        in_specs=(rows, rows, P(None, "fs"), P(None, "fs"), P(None, "fs")),
        out_specs=(rows, tall, tall, tall),
        check_vma=False,
    )
```

```python
import functools
import heapq

import jax
import jax.numpy as jnp
from jax import lax
from jax.experimental import pallas as pl
from jax.experimental.pallas import tpu as pltpu
from jax.sharding import PartitionSpec as P

MESH = pl.DeviceIdType.MESH
F32 = jnp.float32
BF16 = jnp.bfloat16
VMEM_LIMIT = 56 * 1024 * 1024

NY, NZ = 4, 8
X_BEGIN, X_MIDDLE, X_END = 6.0, 14.0, 26.0
BLOCKS = ((0, 256, "z", "r"), (256, 256, "z", "r"), (512, 128, "y", "t"), (640, 128, "y", "t"), (768, 128, "y", "t"), (896, 256, "y", "t"))


Y_RING = ((1, 0, ((2, 1), (1, 1))), (-1, 1, ((2, 1), (1, 1))), (1, 1, ((1, 1),)), (-1, 0, ((1, 1),)))
Z_RING = (
    (1, 0, ((4, 1), (3, 1), (2, 1), (1, 1))), (-1, 1, ((4, 1), (3, 1), (2, 1), (1, 1))),
    (1, 1, ((3, 1), (2, 1), (1, 1))), (-1, 0, ((3, 1), (2, 1), (1, 1))),
)
Z_TWO = (
    (1, 0, ((4, 2), (2, 2))), (-1, 1, ((4, 2), (2, 2))),
    (1, 0, ((3, 2), (1, 1))), (1, 1, ((3, 2), (1, 1))),
    (-1, 0, ((3, 2), (1, 1))), (-1, 1, ((3, 2), (1, 1))),
    (1, 1, ((2, 2),)), (-1, 0, ((2, 2),)),
)
CHAINS = {("y", "r"): Y_RING, ("z", "r"): Z_RING, ("z", "t"): Z_TWO}
OFFSETS = (4, 3, -3, 2, -2, 1, -1, 0)
SLAB = {offset: r for r, offset in enumerate(OFFSETS)}
SLAB[-4] = 0


class Ring:
    def __init__(self, block, phase, axis, style, first_slot):
        self.block, self.phase, self.axis = block, phase, axis
        self.chains = CHAINS[axis, style]
        self.slots, at = {}, 0
        for c, (_, _, hops) in enumerate(self.chains):
            for i in range(len(hops)):
                self.slots[c, i] = at
                at += 1
        self.count, self.first_slot = at, first_slot

    def half_shape(self):
        width = BLOCKS[self.block][1]
        if self.phase == 2:
            return (32, width)
        return (NZ // 2, 64, width) if self.axis == "y" else (NY // 2, 64, width)

    def half_bytes(self):
        size = 2
        for extent in self.half_shape():
            size *= extent
        return size

    def last(self, c):
        return self.slots[c, len(self.chains[c][2]) - 1]

    def ready(self, c):
        _, half, hops = self.chains[c]
        if self.axis == "y":
            return 3 if half == 0 else 7
        return SLAB[self.chains[c][0] * hops[0][0]]


def all_rings():
    rings, slot = {}, 0
    for b, (_, _, first, style) in enumerate(BLOCKS):
        for phase, axis in ((1, first), (2, "z" if first == "y" else "y")):
            rings[b, phase] = Ring(b, phase, axis, "r" if phase == 1 else style, slot)
            slot += rings[b, phase].count
    return rings, slot


def first_sends(rings):
    groups = [[] for _ in OFFSETS]
    for b in range(len(BLOCKS)):
        ring = rings[b, 1]
        for c in range(len(ring.chains)):
            groups[ring.ready(c)].append((b, c))
    return groups


def schedule(rings, rate=46.0e3, latency=3.0, hop=0.75, step=0.06, slab=0.36):
    free, arrivals, order, left, tick = {}, [], [], {}, [0]

    def send(key, c, i, now):
        ring = rings[key]
        sign, _, hops = ring.chains[c]
        link = (ring.axis, sign)
        wire = ring.half_bytes() / rate
        start = max(free.get(link, 0.0), now)
        free[link] = start + wire * hops[i][1]
        tick[0] += 1
        heapq.heappush(arrivals, (start + wire + latency + hop * (hops[i][1] - 1), tick[0], key, c, i))

    for key in rings:
        left[key] = len(rings[key].chains)
    for r, group in enumerate(first_sends(rings)):
        for b, c in group:
            send((b, 1), c, 0, slab * (r + 1))
    now = 0.0
    while arrivals:
        at, _, key, c, i = heapq.heappop(arrivals)
        now = max(now, at) + step
        order.append((now, key, c, i))
        if i + 1 < len(rings[key].chains[c][2]):
            send(key, c, i + 1, now)
        else:
            left[key] -= 1
            if left[key] == 0 and key[1] == 1:
                for k in range(len(rings[key[0], 2].chains)):
                    send((key[0], 2), k, 0, now)
    return order, now


def kernel(tok_hbm, cot_hbm, wg_hbm, wu_hbm, wd_hbm,
           ig_out, gate_out, up_out, down_out,
           xb, wgu, wd, gub, hid, acc, own_ig, ig_part, ig_send0, ig_send, ig_recv0, ig_recv,
           xr1, xr2, *rest):
    nb = len(BLOCKS)
    blks, rest = rest[:nb], rest[nb:]
    rings, total_slots = all_rings()
    keys = [(b, phase) for b in range(nb) for phase in (1, 2)]
    rbufs, rest = dict(zip(keys, rest[: 2 * nb])), rest[2 * nb :]
    fins, rest = rest[:nb], rest[nb:]
    finr, rest = rest[:nb], rest[nb:]
    (load_sem, ag_send, ag_recv, rel_send, rel_recv, igx_send, igx_recv,
     xrs_send, xrs_recv, ring_send, ring_recv, fin_send, fin_recv) = rest

    rep, x, core = lax.axis_index("rep"), lax.axis_index("fs"), lax.axis_index("tp")
    z, y = rep // NY, lax.rem(rep, NY)
    right = (rep, lax.rem(x + 1, 4), core)
    left = (rep, lax.rem(x + 3, 4), core)
    partner = (rep, x, 1 - core)
    far = any(ring.chains is Z_TWO for ring in rings.values())
    y_of = {s: (z * NY + lax.rem(y + s + NY, NY), x, core) for s in (1, -1)}
    z_of = {s: (lax.rem(z + s + NZ, NZ) * NY + y, x, core)
            for s in ((1, -1, 2, -2) if far else (1, -1))}

    def remote(src, dst, send_sem, recv_sem, to):
        return pltpu.make_async_remote_copy(src_ref=src, dst_ref=dst, send_sem=send_sem,
                                            recv_sem=recv_sem, device_id=to, device_id_type=MESH)

    cols = pl.ds(pl.multiple_of(core * 384, 128), 384)
    load_tok = pltpu.make_async_copy(tok_hbm, xb.at[0, 0], load_sem.at[0])
    load_cot = pltpu.make_async_copy(cot_hbm, xb.at[0, 1], load_sem.at[1])
    load_w = [
        pltpu.make_async_copy(wg_hbm.at[:, cols], wgu.at[:, pl.ds(0, 384)], load_sem.at[2]),
        pltpu.make_async_copy(wu_hbm.at[:, cols], wgu.at[:, pl.ds(384, 384)], load_sem.at[3]),
        pltpu.make_async_copy(wd_hbm.at[:, cols], wd, load_sem.at[4]),
    ]
    load_tok.start()
    load_cot.start()
    for copy in load_w:
        copy.start()

    barrier = pltpu.get_barrier_semaphore()
    others = (right, left, partner, *y_of.values(), *z_of.values())
    for other in others:
        pl.semaphore_signal(barrier, inc=1, device_id=other, device_id_type=MESH)
    pl.semaphore_wait(barrier, len(others))
    load_tok.wait()
    load_cot.wait()

    def own_piece(k, side):
        piece = k if side == 0 else (k + 2) % 4
        return remote(xb.at[0, :, pl.ds(32 * piece, 32)], xb.at[2 + k, :, pl.ds(32 * side, 32)],
                      ag_send.at[side, k], ag_recv.at[side, k], right if side == 0 else left)

    def passed_on(k, side):
        return remote(xb.at[2 + k, :, pl.ds(32 * side, 32)], xb.at[6 + k, :, pl.ds(32 * side, 32)],
                      ag_send.at[side, 4 + k], ag_recv.at[side, 4 + k], right if side == 0 else left)

    def arrival(k, side):
        here = xb.at[2 + k, :, pl.ds(32 * side, 32)]
        return remote(here, here, ag_send.at[side, k], ag_recv.at[side, k],
                      right if side == 0 else left)

    def relay(k):
        return remote(xb.at[2 + k, :, pl.ds(0, 64)], xb.at[2 + k, :, pl.ds(64, 64)],
                      rel_send.at[k], rel_recv.at[k], partner)

    own_to_partner = remote(xb.at[0], xb.at[1], rel_send.at[6], rel_recv.at[6], partner)
    for k in range(4):
        for side in (0, 1):
            own_piece(k, side).start()
        if k == 0:
            own_to_partner.start()
    for copy in load_w:
        copy.wait()

    def forward(s):
        rows = pl.ds(pl.multiple_of(s * 128, 128), 128)
        gu = jnp.dot(xb[s, 0], wgu[...], preferred_element_type=F32)
        hg = jnp.dot(xb[s, 1], wd[...], preferred_element_type=F32)
        gate, up = gu[:, :384], gu[:, 384:]
        sig = jax.nn.sigmoid(gate)
        act = gate * sig
        gub[rows, pl.ds(0, 384)] = (hg * up * sig * (1.0 + gate * (1.0 - sig))).astype(BF16)
        gub[rows, pl.ds(384, 384)] = (hg * act).astype(BF16)
        hid[rows, :] = (act * up).astype(BF16)

    def input_part(s, store):
        rows = pl.ds(pl.multiple_of(s * 128, 128), 128)

        def some(n, carry):
            d = pl.ds(pl.multiple_of(n * 512, 512), 512)
            part = lax.dot_general(gub[rows, :], wgu[d, :], (((1,), (1,)), ((), ())),
                                   preferred_element_type=F32)
            store(d, part.astype(BF16))
            return carry

        lax.fori_loop(0, 4, some, 0)

    def store_own(d, part):
        own_ig[:, d] = part

    def store_partner(d, part):
        ig_send0[:, d] = part

    send_ig0 = remote(ig_send0, ig_recv0, igx_send.at[6], igx_recv.at[6], partner)

    def send_ig(k):
        return remote(ig_send.at[k], ig_recv.at[k], igx_send.at[k], igx_recv.at[k], partner)

    def step_part(s):
        k = s - 2

        def store(d, part):
            ig_part[k, :, d] = part[:64]
            ig_send[k, :, d] = part[64:]

        input_part(s, store)
        send_ig(k).start()

    forward(0)
    input_part(0, store_own)
    own_to_partner.wait_recv()
    forward(1)
    input_part(1, store_partner)
    send_ig0.start()

    def take(k):
        arrival(k, 0).wait_recv()
        arrival(k, 1).wait_recv()
        relay(k).start()

    def early(k, carry):
        take(k)

        @pl.when(k < 2)
        def _():
            passed_on(k, 0).start()
            passed_on(k, 1).start()

        relay(k).wait_recv()
        forward(k + 2)
        step_part(k + 2)
        return carry

    lax.fori_loop(0, 4, early, 0)

    across = (((0,), (0,)), ((), ()))

    def products(j, first, count):
        d = pl.ds(pl.multiple_of(j * 256, 256), 256)
        rows = pl.ds(first * 128, count * 128)
        tok = xb[pl.ds(first, count), 0, :, d].reshape(count * 128, 256)
        cot = xb[pl.ds(first, count), 1, :, d].reshape(count * 128, 256)
        return (lax.dot_general(tok, gub[rows, :], across, preferred_element_type=F32),
                lax.dot_general(cot, hid[rows, :], across, preferred_element_type=F32))

    def first_sums(j, carry):
        a, b = products(j, 0, 6)
        acc[j, :, pl.ds(0, 768)] = a
        acc[j, :, pl.ds(768, 384)] = b
        return carry

    lax.fori_loop(0, 4, first_sums, 0)
    take(4)
    lax.fori_loop(4, 8, first_sums, 0)
    relay(4).wait_recv()
    forward(6)
    take(5)
    step_part(6)
    relay(5).wait_recv()
    forward(7)

    def half_of(ring, offset, half):
        blk = blks[ring.block]
        if ring.axis == "y":
            there = lax.rem(y + offset + NY, NY)
            if ring.phase == 1:
                return blk.at[pl.ds(4 * half, 4), there]
            return blk.at[SLAB[0], there, pl.ds(32 * half, 32)]
        if ring.phase == 1:
            return blk.at[SLAB[offset], pl.ds(2 * half, 2)]
        return blk.at[SLAB[offset], y, pl.ds(32 * half, 32)]

    def hop(key, c, i):
        ring = rings[key]
        sign, half, hops = ring.chains[c]
        slot = ring.slots[c, i]
        sem = ring.first_slot + slot
        return remote(half_of(ring, sign * hops[i][0], half), rbufs[key].at[slot],
                      ring_send.at[sem], ring_recv.at[sem],
                      (y_of if ring.axis == "y" else z_of)[sign * hops[i][1]])

    def add_into(dst, src):
        shape = dst.shape
        if len(shape) == 2:
            dst[...] = (dst[...].astype(F32) + src[...].astype(F32)).astype(BF16)
        else:
            def one(i, carry):
                dst[i] = (dst[i].astype(F32) + src[i].astype(F32)).astype(BF16)
                return carry
            lax.fori_loop(0, shape[0], one, 0)

    for r, group in enumerate(first_sends(rings)):
        j = lax.rem(z + OFFSETS[r] + NZ, NZ)
        a, b = products(j, 6, 2)
        a = (acc[j, :, pl.ds(0, 768)] + a).astype(BF16)
        b = (acc[j, :, pl.ds(768, 384)] + b).astype(BF16)
        for i, (col, width, _, _) in enumerate(BLOCKS):
            piece = a[:, col : col + width] if col < 768 else b[:, col - 768 : col - 768 + width]
            blks[i][r] = piece.reshape(NY, 64, width)
        for block, c in group:
            hop((block, 1), c, 0).start()

    step_part(7)

    def xrs(stage, way):
        rows = pl.ds(32 * way, 32)
        which = {0: (4, 2), 1: (2, 2), 2: (0, 2)}[stage]
        dst = xr1.at[way] if stage == 0 else xr2.at[way, pl.ds(which[0], 2)]
        return remote(ig_part.at[pl.ds(which[0], 2), rows], dst, xrs_send.at[stage, way],
                      xrs_recv.at[stage, way], left if way == 0 else right)

    def merge_part(k, carry):
        send_ig(k).wait_recv()
        ig_part[k] = (ig_part[k].astype(F32) + ig_recv[k].astype(F32)).astype(BF16)
        return carry

    def x_begin():
        lax.fori_loop(2, 6, merge_part, 0)
        for stage in (0, 1):
            for way in (0, 1):
                xrs(stage, way).start()
        lax.fori_loop(0, 2, merge_part, 0)
        send_ig0.wait_recv()

    def x_middle():
        for way in (0, 1):
            xrs(0, way).wait_recv()
        for k in range(2):
            for way in (0, 1):
                rows = pl.ds(32 * way, 32)
                ig_part[k, rows, :] = (ig_part[k, rows, :].astype(F32)
                                       + xr1[way, k].astype(F32)).astype(BF16)
        for way in (0, 1):
            xrs(2, way).start()

    def x_end():
        for stage in (1, 2):
            for way in (0, 1):
                xrs(stage, way).wait_recv()
        for piece in range(4):
            rows = pl.ds(32 * piece, 32)
            total = own_ig[rows, :].astype(F32) + ig_recv0[rows, :].astype(F32)
            total = total + xr2[0, piece].astype(F32) + xr2[1, (piece + 2) % 4].astype(F32)
            ig_out[rows, :] = total.astype(BF16)

    order, _ = schedule(rings)
    left_of = {key: len(rings[key].chains) for key in keys}
    scale = float(32768) ** -0.5

    def fin_copy(b):
        return remote(fins[b].at[pl.ds(pl.multiple_of((1 - core) * 32, 32), 32)], finr[b],
                      fin_send.at[b], fin_recv.at[b], partner)

    def finish_block(b):
        ring = rings[b, 2]
        for half in (0, 1):
            total = half_of(ring, 0, half)[...].astype(F32)
            for c, (_, h, _) in enumerate(ring.chains):
                if h == half:
                    total = total + rbufs[b, 2][ring.last(c)].astype(F32)
            fins[b][pl.ds(32 * half, 32), :] = total * scale
        fin_copy(b).start()

    todo = [(X_BEGIN, x_begin), (X_MIDDLE, x_middle), (X_END, x_end)]
    for at, key, c, i in order:
        while todo and at > todo[0][0]:
            todo.pop(0)[1]()
        ring = rings[key]
        sign, half, hops = ring.chains[c]
        hop(key, c, i).wait_recv()
        if i + 1 < len(hops):
            add_into(half_of(ring, sign * hops[i + 1][0], half), rbufs[key].at[ring.slots[c, i]])
            hop(key, c, i + 1).start()
        else:
            left_of[key] -= 1
            if key[1] == 1:
                add_into(half_of(ring, 0, half), rbufs[key].at[ring.slots[c, i]])
                if left_of[key] == 0:
                    second = (key[0], 2)
                    for k in range(len(rings[second].chains)):
                        hop(second, k, 0).start()
            elif left_of[key] == 0:
                finish_block(key[0])
    for _, act in todo:
        act()

    def place_out(b, value, which):
        col, width, _, _ = BLOCKS[b]
        at = col
        while at < col + width:
            take_n = min(384 - at % 384, col + width - at)
            out = (gate_out, up_out, down_out)[at // 384]
            out[:, pl.ds(pl.multiple_of(which * 384 + at % 384, 128), take_n)] = (
                value[:, at - col : at - col + take_n])
            at += take_n

    mine = pl.ds(pl.multiple_of(core * 32, 32), 32)
    for b in range(nb):
        place_out(b, fins[b][mine, :], core)
    for b in range(nb):
        fin_copy(b).wait_recv()
        place_out(b, finr[b][...], 1 - core)

    for k in range(4):
        for side in (0, 1):
            own_piece(k, side).wait_send()
    for k in range(2):
        for side in (0, 1):
            passed_on(k, side).wait_send()
    for k in range(6):
        relay(k).wait_send()
        send_ig(k).wait_send()
    own_to_partner.wait_send()
    send_ig0.wait_send()
    for stage in range(3):
        for way in (0, 1):
            xrs(stage, way).wait_send()
    for _, key, c, i in order:
        hop(key, c, i).wait_send()
    for b in range(nb):
        fin_copy(b).wait_send()


def write_out(a, b, c, d, out_a, out_b, out_c, out_d, sems):
    copies = [pltpu.make_async_copy(src, dst, sems.at[i])
              for i, (src, dst) in enumerate(((a, out_a), (b, out_b), (c, out_c), (d, out_d)))]
    for copy in copies:
        copy.start()
    for copy in copies:
        copy.wait()


def on_device(tokens, cotangent, gate_weight, up_weight, down_weight_t):
    rings, slots = all_rings()
    keys = [(b, phase) for b in range(len(BLOCKS)) for phase in (1, 2)]
    anywhere = pl.BlockSpec(memory_space=pl.ANY)
    vmem = pl.BlockSpec(memory_space=pltpu.VMEM)
    dma = pltpu.SemaphoreType.DMA
    results = pl.pallas_call(
        kernel,
        out_shape=(
            jax.ShapeDtypeStruct((128, 2048), BF16),
            jax.ShapeDtypeStruct((32, 768), F32),
            jax.ShapeDtypeStruct((32, 768), F32),
            jax.ShapeDtypeStruct((32, 768), F32),
        ),
        in_specs=[anywhere] * 5,
        out_specs=[vmem] * 4,
        scratch_shapes=[
            pltpu.VMEM((8, 2, 128, 2048), BF16),
            pltpu.VMEM((2048, 768), BF16),
            pltpu.VMEM((2048, 384), BF16),
            pltpu.VMEM((1024, 768), BF16),
            pltpu.VMEM((1024, 384), BF16),
            pltpu.VMEM((8, 256, 1152), F32),
            pltpu.VMEM((128, 2048), BF16),
            pltpu.VMEM((6, 64, 2048), BF16),
            pltpu.VMEM((128, 2048), BF16),
            pltpu.VMEM((6, 64, 2048), BF16),
            pltpu.VMEM((128, 2048), BF16),
            pltpu.VMEM((6, 64, 2048), BF16),
            pltpu.VMEM((2, 2, 32, 2048), BF16),
            pltpu.VMEM((2, 4, 32, 2048), BF16),
        ]
        + [pltpu.VMEM((NZ, NY, 64, width), BF16) for _, width, _, _ in BLOCKS]
        + [pltpu.VMEM((rings[key].count, *rings[key].half_shape()), BF16) for key in keys]
        + [pltpu.VMEM((64, width), F32) for _, width, _, _ in BLOCKS]
        + [pltpu.VMEM((32, width), F32) for _, width, _, _ in BLOCKS]
        + [
            dma((5,)), dma((2, 6)), dma((2, 6)), dma((7,)), dma((7,)), dma((7,)), dma((7,)),
            dma((3, 2)), dma((3, 2)), dma((slots,)), dma((slots,)),
            dma((len(BLOCKS),)), dma((len(BLOCKS),)),
        ],
        compiler_params=pltpu.CompilerParams(
            collective_id=0, has_side_effects=True, vmem_limit_bytes=VMEM_LIMIT
        ),
    )(tokens, cotangent, gate_weight, up_weight, down_weight_t)
    return pl.pallas_call(
        write_out,
        out_shape=tuple(jax.ShapeDtypeStruct(r.shape, r.dtype) for r in results),
        in_specs=[vmem] * 4,
        out_specs=[anywhere] * 4,
        scratch_shapes=[dma((4,))],
        compiler_params=pltpu.CompilerParams(vmem_limit_bytes=4 * 1024 * 1024),
    )(*results)


def solution(mesh):
    rows, tall = P(("rep", "fs", "tp"), None), P(("rep", "tp"), "fs")
    return jax.shard_map(
        on_device,
        mesh=mesh,
        in_specs=(rows, rows, P(None, "fs"), P(None, "fs"), P(None, "fs")),
        out_specs=(rows, tall, tall, tall),
        check_vma=False,
    )
```

```python
import functools
import heapq

import jax
import jax.numpy as jnp
from jax import lax
from jax.experimental import pallas as pl
from jax.experimental.pallas import tpu as pltpu
from jax.sharding import PartitionSpec as P

MESH = pl.DeviceIdType.MESH
F32 = jnp.float32
BF16 = jnp.bfloat16
VMEM_LIMIT = 56 * 1024 * 1024

NY, NZ = 4, 8
X_BEGIN, X_MIDDLE, X_END = 6.0, 14.0, 26.0
BLOCKS = ((0, 256, "z", "r"), (256, 256, "z", "r"), (512, 128, "y", "t"), (640, 128, "y", "t"), (768, 128, "y", "t"), (896, 256, "y", "t"))


Y_RING = ((1, 0, ((2, 1), (1, 1))), (-1, 1, ((2, 1), (1, 1))), (1, 1, ((1, 1),)), (-1, 0, ((1, 1),)))
Z_RING = (
    (1, 0, ((4, 1), (3, 1), (2, 1), (1, 1))), (-1, 1, ((4, 1), (3, 1), (2, 1), (1, 1))),
    (1, 1, ((3, 1), (2, 1), (1, 1))), (-1, 0, ((3, 1), (2, 1), (1, 1))),
)
Z_TWO = (
    (1, 0, ((4, 2), (2, 2))), (-1, 1, ((4, 2), (2, 2))),
    (1, 0, ((3, 2), (1, 1))), (1, 1, ((3, 2), (1, 1))),
    (-1, 0, ((3, 2), (1, 1))), (-1, 1, ((3, 2), (1, 1))),
    (1, 1, ((2, 2),)), (-1, 0, ((2, 2),)),
)
CHAINS = {("y", "r"): Y_RING, ("z", "r"): Z_RING, ("z", "t"): Z_TWO}
OFFSETS = (4, 3, -3, 2, -2, 1, -1, 0)
SLAB = {offset: r for r, offset in enumerate(OFFSETS)}
SLAB[-4] = 0


class Ring:
    def __init__(self, block, phase, axis, style, first_slot):
        self.block, self.phase, self.axis = block, phase, axis
        self.chains = CHAINS[axis, style]
        self.slots, at = {}, 0
        for c, (_, _, hops) in enumerate(self.chains):
            for i in range(len(hops)):
                self.slots[c, i] = at
                at += 1
        self.count, self.first_slot = at, first_slot

    def half_shape(self):
        width = BLOCKS[self.block][1]
        if self.phase == 2:
            return (32, width)
        return (NZ // 2, 64, width) if self.axis == "y" else (NY // 2, 64, width)

    def half_bytes(self):
        size = 2
        for extent in self.half_shape():
            size *= extent
        return size

    def last(self, c):
        return self.slots[c, len(self.chains[c][2]) - 1]

    def ready(self, c):
        _, half, hops = self.chains[c]
        if self.axis == "y":
            return 3 if half == 0 else 7
        return SLAB[self.chains[c][0] * hops[0][0]]


def all_rings():
    rings, slot = {}, 0
    for b, (_, _, first, style) in enumerate(BLOCKS):
        for phase, axis in ((1, first), (2, "z" if first == "y" else "y")):
            rings[b, phase] = Ring(b, phase, axis, "r" if phase == 1 else style, slot)
            slot += rings[b, phase].count
    return rings, slot


def first_sends(rings):
    groups = [[] for _ in OFFSETS]
    for b in range(len(BLOCKS)):
        ring = rings[b, 1]
        for c in range(len(ring.chains)):
            groups[ring.ready(c)].append((b, c))
    return groups


def schedule(rings, rate=46.0e3, latency=3.0, hop=0.75, step=0.06, slab=0.36):
    free, arrivals, order, left, tick = {}, [], [], {}, [0]

    def send(key, c, i, now):
        ring = rings[key]
        sign, _, hops = ring.chains[c]
        link = (ring.axis, sign)
        wire = ring.half_bytes() / rate
        start = max(free.get(link, 0.0), now)
        free[link] = start + wire * hops[i][1]
        tick[0] += 1
        heapq.heappush(arrivals, (start + wire + latency + hop * (hops[i][1] - 1), tick[0], key, c, i))

    for key in rings:
        left[key] = len(rings[key].chains)
    for r, group in enumerate(first_sends(rings)):
        for b, c in group:
            send((b, 1), c, 0, slab * (r + 1))
    now = 0.0
    while arrivals:
        at, _, key, c, i = heapq.heappop(arrivals)
        now = max(now, at) + step
        order.append((now, key, c, i))
        if i + 1 < len(rings[key].chains[c][2]):
            send(key, c, i + 1, now)
        else:
            left[key] -= 1
            if left[key] == 0 and key[1] == 1:
                for k in range(len(rings[key[0], 2].chains)):
                    send((key[0], 2), k, 0, now)
    return order, now


def kernel(tok_hbm, cot_hbm, wg_hbm, wu_hbm, wd_hbm,
           ig_out, gate_out, up_out, down_out,
           xb, wgu, wd, gub, hid, acc, own_ig, ig_part, ig_send0, ig_send, ig_recv0, ig_recv,
           xr1, xr2, *rest):
    nb = len(BLOCKS)
    blks, rest = rest[:nb], rest[nb:]
    rings, total_slots = all_rings()
    keys = [(b, phase) for b in range(nb) for phase in (1, 2)]
    rbufs, rest = dict(zip(keys, rest[: 2 * nb])), rest[2 * nb :]
    fins, rest = rest[:nb], rest[nb:]
    finr, rest = rest[:nb], rest[nb:]
    (load_sem, ag_send, ag_recv, rel_send, rel_recv, igx_send, igx_recv,
     xrs_send, xrs_recv, ring_send, ring_recv, fin_send, fin_recv) = rest

    rep, x, core = lax.axis_index("rep"), lax.axis_index("fs"), lax.axis_index("tp")
    z, y = rep // NY, lax.rem(rep, NY)
    right = (rep, lax.rem(x + 1, 4), core)
    left = (rep, lax.rem(x + 3, 4), core)
    partner = (rep, x, 1 - core)
    far = any(ring.chains is Z_TWO for ring in rings.values())
    y_of = {s: (z * NY + lax.rem(y + s + NY, NY), x, core) for s in (1, -1)}
    z_of = {s: (lax.rem(z + s + NZ, NZ) * NY + y, x, core)
            for s in ((1, -1, 2, -2) if far else (1, -1))}

    def remote(src, dst, send_sem, recv_sem, to):
        return pltpu.make_async_remote_copy(src_ref=src, dst_ref=dst, send_sem=send_sem,
                                            recv_sem=recv_sem, device_id=to, device_id_type=MESH)

    cols = pl.ds(pl.multiple_of(core * 384, 128), 384)
    load_tok = pltpu.make_async_copy(tok_hbm, xb.at[0, 0], load_sem.at[0])
    load_cot = pltpu.make_async_copy(cot_hbm, xb.at[0, 1], load_sem.at[1])
    load_w = [
        pltpu.make_async_copy(wg_hbm.at[:, cols], wgu.at[:, pl.ds(0, 384)], load_sem.at[2]),
        pltpu.make_async_copy(wu_hbm.at[:, cols], wgu.at[:, pl.ds(384, 384)], load_sem.at[3]),
        pltpu.make_async_copy(wd_hbm.at[:, cols], wd, load_sem.at[4]),
    ]
    load_tok.start()
    load_cot.start()
    for copy in load_w:
        copy.start()

    barrier = pltpu.get_barrier_semaphore()
    others = (right, left, partner, *y_of.values(), *z_of.values())
    for other in others:
        pl.semaphore_signal(barrier, inc=1, device_id=other, device_id_type=MESH)
    pl.semaphore_wait(barrier, len(others))
    load_tok.wait()
    load_cot.wait()

    def own_piece(k, side):
        piece = k if side == 0 else (k + 2) % 4
        return remote(xb.at[0, :, pl.ds(32 * piece, 32)], xb.at[2 + k, :, pl.ds(32 * side, 32)],
                      ag_send.at[side, k], ag_recv.at[side, k], right if side == 0 else left)

    def passed_on(k, side):
        return remote(xb.at[2 + k, :, pl.ds(32 * side, 32)], xb.at[6 + k, :, pl.ds(32 * side, 32)],
                      ag_send.at[side, 4 + k], ag_recv.at[side, 4 + k], right if side == 0 else left)

    def arrival(k, side):
        here = xb.at[2 + k, :, pl.ds(32 * side, 32)]
        return remote(here, here, ag_send.at[side, k], ag_recv.at[side, k],
                      right if side == 0 else left)

    def relay(k):
        return remote(xb.at[2 + k, :, pl.ds(0, 64)], xb.at[2 + k, :, pl.ds(64, 64)],
                      rel_send.at[k], rel_recv.at[k], partner)

    own_to_partner = remote(xb.at[0], xb.at[1], rel_send.at[6], rel_recv.at[6], partner)
    for k in range(4):
        for side in (0, 1):
            own_piece(k, side).start()
        if k == 0:
            own_to_partner.start()
    for copy in load_w:
        copy.wait()

    def forward(s):
        rows = pl.ds(pl.multiple_of(s * 128, 128), 128)
        gu = jnp.dot(xb[s, 0], wgu[...], preferred_element_type=F32)
        hg = jnp.dot(xb[s, 1], wd[...], preferred_element_type=F32)
        gate, up = gu[:, :384], gu[:, 384:]
        sig = jax.nn.sigmoid(gate)
        act = gate * sig
        gub[rows, pl.ds(0, 384)] = (hg * up * sig * (1.0 + gate * (1.0 - sig))).astype(BF16)
        gub[rows, pl.ds(384, 384)] = (hg * act).astype(BF16)
        hid[rows, :] = (act * up).astype(BF16)

    def input_part(s, store):
        rows = pl.ds(pl.multiple_of(s * 128, 128), 128)

        def some(n, carry):
            d = pl.ds(pl.multiple_of(n * 512, 512), 512)
            part = lax.dot_general(gub[rows, :], wgu[d, :], (((1,), (1,)), ((), ())),
                                   preferred_element_type=F32)
            store(d, part.astype(BF16))
            return carry

        lax.fori_loop(0, 4, some, 0)

    def store_own(d, part):
        own_ig[:, d] = part

    def store_partner(d, part):
        ig_send0[:, d] = part

    send_ig0 = remote(ig_send0, ig_recv0, igx_send.at[6], igx_recv.at[6], partner)

    def send_ig(k):
        return remote(ig_send.at[k], ig_recv.at[k], igx_send.at[k], igx_recv.at[k], partner)

    def step_part(s):
        k = s - 2

        def store(d, part):
            ig_part[k, :, d] = part[:64]
            ig_send[k, :, d] = part[64:]

        input_part(s, store)
        send_ig(k).start()

    forward(0)
    input_part(0, store_own)
    own_to_partner.wait_recv()
    forward(1)
    input_part(1, store_partner)
    send_ig0.start()

    def take(k):
        arrival(k, 0).wait_recv()
        arrival(k, 1).wait_recv()
        relay(k).start()

    def early(k, carry):
        take(k)

        @pl.when(k < 2)
        def _():
            passed_on(k, 0).start()
            passed_on(k, 1).start()

        relay(k).wait_recv()
        forward(k + 2)
        step_part(k + 2)
        return carry

    lax.fori_loop(0, 4, early, 0)

    across = (((0,), (0,)), ((), ()))

    def products(j, first, count):
        d = pl.ds(pl.multiple_of(j * 256, 256), 256)
        rows = pl.ds(first * 128, count * 128)
        tok = xb[pl.ds(first, count), 0, :, d].reshape(count * 128, 256)
        cot = xb[pl.ds(first, count), 1, :, d].reshape(count * 128, 256)
        return (lax.dot_general(tok, gub[rows, :], across, preferred_element_type=F32),
                lax.dot_general(cot, hid[rows, :], across, preferred_element_type=F32))

    def first_sums(j, carry):
        a, b = products(j, 0, 6)
        acc[j, :, pl.ds(0, 768)] = a
        acc[j, :, pl.ds(768, 384)] = b
        return carry

    lax.fori_loop(0, 4, first_sums, 0)
    take(4)
    lax.fori_loop(4, 8, first_sums, 0)
    relay(4).wait_recv()
    forward(6)
    take(5)
    step_part(6)
    relay(5).wait_recv()
    forward(7)

    def half_of(ring, offset, half):
        blk = blks[ring.block]
        if ring.axis == "y":
            there = lax.rem(y + offset + NY, NY)
            if ring.phase == 1:
                return blk.at[pl.ds(4 * half, 4), there]
            return blk.at[SLAB[0], there, pl.ds(32 * half, 32)]
        if ring.phase == 1:
            return blk.at[SLAB[offset], pl.ds(2 * half, 2)]
        return blk.at[SLAB[offset], y, pl.ds(32 * half, 32)]

    def hop(key, c, i):
        ring = rings[key]
        sign, half, hops = ring.chains[c]
        slot = ring.slots[c, i]
        sem = ring.first_slot + slot
        return remote(half_of(ring, sign * hops[i][0], half), rbufs[key].at[slot],
                      ring_send.at[sem], ring_recv.at[sem],
                      (y_of if ring.axis == "y" else z_of)[sign * hops[i][1]])

    def add_into(dst, src):
        shape = dst.shape
        if len(shape) == 2:
            dst[...] = (dst[...].astype(F32) + src[...].astype(F32)).astype(BF16)
        else:
            def one(i, carry):
                dst[i] = (dst[i].astype(F32) + src[i].astype(F32)).astype(BF16)
                return carry
            lax.fori_loop(0, shape[0], one, 0)

    for r, group in enumerate(first_sends(rings)):
        j = lax.rem(z + OFFSETS[r] + NZ, NZ)
        a, b = products(j, 6, 2)
        a = (acc[j, :, pl.ds(0, 768)] + a).astype(BF16)
        b = (acc[j, :, pl.ds(768, 384)] + b).astype(BF16)
        for i, (col, width, _, _) in enumerate(BLOCKS):
            piece = a[:, col : col + width] if col < 768 else b[:, col - 768 : col - 768 + width]
            blks[i][r] = piece.reshape(NY, 64, width)
        for block, c in group:
            hop((block, 1), c, 0).start()

    step_part(7)

    def xrs(stage, way):
        rows = pl.ds(32 * way, 32)
        which = {0: (4, 2), 1: (2, 2), 2: (0, 2)}[stage]
        dst = xr1.at[way] if stage == 0 else xr2.at[way, pl.ds(which[0], 2)]
        return remote(ig_part.at[pl.ds(which[0], 2), rows], dst, xrs_send.at[stage, way],
                      xrs_recv.at[stage, way], left if way == 0 else right)

    def merge_part(k, carry):
        send_ig(k).wait_recv()
        ig_part[k] = (ig_part[k].astype(F32) + ig_recv[k].astype(F32)).astype(BF16)
        return carry

    def x_begin():
        lax.fori_loop(2, 6, merge_part, 0)
        for stage in (0, 1):
            for way in (0, 1):
                xrs(stage, way).start()
        lax.fori_loop(0, 2, merge_part, 0)
        send_ig0.wait_recv()

    def x_middle():
        for way in (0, 1):
            xrs(0, way).wait_recv()
        for k in range(2):
            for way in (0, 1):
                rows = pl.ds(32 * way, 32)
                ig_part[k, rows, :] = (ig_part[k, rows, :].astype(F32)
                                       + xr1[way, k].astype(F32)).astype(BF16)
        for way in (0, 1):
            xrs(2, way).start()

    def x_end():
        for stage in (1, 2):
            for way in (0, 1):
                xrs(stage, way).wait_recv()
        for piece in range(4):
            rows = pl.ds(32 * piece, 32)
            total = own_ig[rows, :].astype(F32) + ig_recv0[rows, :].astype(F32)
            total = total + xr2[0, piece].astype(F32) + xr2[1, (piece + 2) % 4].astype(F32)
            ig_out[rows, :] = total.astype(BF16)

    order, _ = schedule(rings)
    left_of = {key: len(rings[key].chains) for key in keys}
    scale = float(32768) ** -0.5

    def fin_copy(b):
        return remote(fins[b].at[pl.ds(pl.multiple_of((1 - core) * 32, 32), 32)], finr[b],
                      fin_send.at[b], fin_recv.at[b], partner)

    def finish_block(b):
        ring = rings[b, 2]
        for half in (0, 1):
            total = half_of(ring, 0, half)[...].astype(F32)
            for c, (_, h, _) in enumerate(ring.chains):
                if h == half:
                    total = total + rbufs[b, 2][ring.last(c)].astype(F32)
            fins[b][pl.ds(32 * half, 32), :] = total * scale
        fin_copy(b).start()

    todo = [(X_BEGIN, x_begin), (X_MIDDLE, x_middle), (X_END, x_end)]
    for at, key, c, i in order:
        while todo and at > todo[0][0]:
            todo.pop(0)[1]()
        ring = rings[key]
        sign, half, hops = ring.chains[c]
        hop(key, c, i).wait_recv()
        if i + 1 < len(hops):
            add_into(half_of(ring, sign * hops[i + 1][0], half), rbufs[key].at[ring.slots[c, i]])
            hop(key, c, i + 1).start()
        else:
            left_of[key] -= 1
            if key[1] == 1:
                add_into(half_of(ring, 0, half), rbufs[key].at[ring.slots[c, i]])
                if left_of[key] == 0:
                    second = (key[0], 2)
                    for k in range(len(rings[second].chains)):
                        hop(second, k, 0).start()
            elif left_of[key] == 0:
                finish_block(key[0])
    for _, act in todo:
        act()

    def place_out(b, value, which):
        col, width, _, _ = BLOCKS[b]
        at = col
        while at < col + width:
            take_n = min(384 - at % 384, col + width - at)
            out = (gate_out, up_out, down_out)[at // 384]
            out[:, pl.ds(pl.multiple_of(which * 384 + at % 384, 128), take_n)] = (
                value[:, at - col : at - col + take_n])
            at += take_n

    mine = pl.ds(pl.multiple_of(core * 32, 32), 32)
    for b in range(nb):
        place_out(b, fins[b][mine, :], core)
    for b in range(nb):
        fin_copy(b).wait_recv()
        place_out(b, finr[b][...], 1 - core)

    for k in range(4):
        for side in (0, 1):
            own_piece(k, side).wait_send()
    for k in range(2):
        for side in (0, 1):
            passed_on(k, side).wait_send()
    for k in range(6):
        relay(k).wait_send()
        send_ig(k).wait_send()
    own_to_partner.wait_send()
    send_ig0.wait_send()
    for stage in range(3):
        for way in (0, 1):
            xrs(stage, way).wait_send()
    for _, key, c, i in order:
        hop(key, c, i).wait_send()
    for b in range(nb):
        fin_copy(b).wait_send()


def write_out(a, b, c, d, out_a, out_b, out_c, out_d, sems):
    copies = [pltpu.make_async_copy(src, dst, sems.at[i])
              for i, (src, dst) in enumerate(((a, out_a), (b, out_b), (c, out_c), (d, out_d)))]
    for copy in copies:
        copy.start()
    for copy in copies:
        copy.wait()


def on_device(tokens, cotangent, gate_weight, up_weight, down_weight_t):
    rings, slots = all_rings()
    keys = [(b, phase) for b in range(len(BLOCKS)) for phase in (1, 2)]
    anywhere = pl.BlockSpec(memory_space=pl.ANY)
    vmem = pl.BlockSpec(memory_space=pltpu.VMEM)
    dma = pltpu.SemaphoreType.DMA
    results = pl.pallas_call(
        kernel,
        out_shape=(
            pltpu.VMEM((128, 2048), BF16),
            pltpu.VMEM((32, 768), F32),
            pltpu.VMEM((32, 768), F32),
            pltpu.VMEM((32, 768), F32),
        ),
        in_specs=[anywhere] * 5,
        out_specs=[vmem] * 4,
        scratch_shapes=[
            pltpu.VMEM((8, 2, 128, 2048), BF16),
            pltpu.VMEM((2048, 768), BF16),
            pltpu.VMEM((2048, 384), BF16),
            pltpu.VMEM((1024, 768), BF16),
            pltpu.VMEM((1024, 384), BF16),
            pltpu.VMEM((8, 256, 1152), F32),
            pltpu.VMEM((128, 2048), BF16),
            pltpu.VMEM((6, 64, 2048), BF16),
            pltpu.VMEM((128, 2048), BF16),
            pltpu.VMEM((6, 64, 2048), BF16),
            pltpu.VMEM((128, 2048), BF16),
            pltpu.VMEM((6, 64, 2048), BF16),
            pltpu.VMEM((2, 2, 32, 2048), BF16),
            pltpu.VMEM((2, 4, 32, 2048), BF16),
        ]
        + [pltpu.VMEM((NZ, NY, 64, width), BF16) for _, width, _, _ in BLOCKS]
        + [pltpu.VMEM((rings[key].count, *rings[key].half_shape()), BF16) for key in keys]
        + [pltpu.VMEM((64, width), F32) for _, width, _, _ in BLOCKS]
        + [pltpu.VMEM((32, width), F32) for _, width, _, _ in BLOCKS]
        + [
            dma((5,)), dma((2, 6)), dma((2, 6)), dma((7,)), dma((7,)), dma((7,)), dma((7,)),
            dma((3, 2)), dma((3, 2)), dma((slots,)), dma((slots,)),
            dma((len(BLOCKS),)), dma((len(BLOCKS),)),
        ],
        compiler_params=pltpu.CompilerParams(
            collective_id=0, has_side_effects=True, vmem_limit_bytes=VMEM_LIMIT
        ),
    )(tokens, cotangent, gate_weight, up_weight, down_weight_t)
    return pl.pallas_call(
        write_out,
        out_shape=tuple(jax.ShapeDtypeStruct(r.shape, r.dtype) for r in results),
        in_specs=[vmem] * 4,
        out_specs=[anywhere] * 4,
        scratch_shapes=[dma((4,))],
        compiler_params=pltpu.CompilerParams(vmem_limit_bytes=4 * 1024 * 1024),
    )(*results)


def solution(mesh):
    rows, tall = P(("rep", "fs", "tp"), None), P(("rep", "tp"), "fs")
    return jax.shard_map(
        on_device,
        mesh=mesh,
        in_specs=(rows, rows, P(None, "fs"), P(None, "fs"), P(None, "fs")),
        out_specs=(rows, tall, tall, tall),
        check_vma=False,
    )
```

```python
import heapq
import itertools

import jax
import jax.numpy as jnp
from jax import lax
from jax.experimental import pallas as pl
from jax.experimental.pallas import tpu as pltpu
from jax.sharding import PartitionSpec as P

MESH = pl.DeviceIdType.MESH
F32 = jnp.float32
BF16 = jnp.bfloat16
VMEM_LIMIT = 56 * 1024 * 1024

NY, NZ = 4, 8
X_BEGIN, X_MIDDLE, X_END = 6.0, 14.0, 26.0
ASIDE = tuple(("part", 0.42, 0.0) for _ in range(8)) + (("begin", 0.45, 8.5), ("middle", 0.15, 18.5), ("end", 0.3, 29.5))
BLOCKS = (
    (
        (0, 256, "z", "d"),
        (256, 256, "z", "r"),
        (768, 128, "y", "t"),
        (512, 256, "y", "m"),
        (896, 128, "y", "t"),
        (1024, 128, "z", "d"),
    ),
    (
        (0, 128, "z", "r"),
        (128, 128, "y", "r"),
        (256, 256, "y", "r"),
        (768, 128, "y", "m"),
        (512, 256, "y", "t"),
        (896, 128, "z", "r"),
        (1024, 128, "z", "r"),
    ),
)
Y_RING = ((1, 0, ((2, 1), (1, 1))), (-1, 1, ((2, 1), (1, 1))), (1, 1, ((1, 1),)), (-1, 0, ((1, 1),)))
Z_RING = (
    (1, 0, ((4, 1), (3, 1), (2, 1), (1, 1))), (-1, 1, ((4, 1), (3, 1), (2, 1), (1, 1))),
    (1, 1, ((3, 1), (2, 1), (1, 1))), (-1, 0, ((3, 1), (2, 1), (1, 1))),
)
Z_TWO = (
    (1, 0, ((4, 2), (2, 2))), (-1, 1, ((4, 2), (2, 2))),
    (1, 0, ((3, 2), (1, 1))), (1, 1, ((3, 2), (1, 1))),
    (-1, 0, ((3, 2), (1, 1))), (-1, 1, ((3, 2), (1, 1))),
    (1, 1, ((2, 2),)), (-1, 0, ((2, 2),)),
)
Z_MID = (
    (1, 0, ((4, 1), (3, 2), (1, 1))), (-1, 1, ((4, 1), (3, 2), (1, 1))),
    (1, 1, ((3, 2), (1, 1))), (-1, 0, ((3, 2), (1, 1))),
    (1, 0, ((2, 2),)), (1, 1, ((2, 2),)), (-1, 0, ((2, 2),)), (-1, 1, ((2, 2),)),
)
Y_DIRECT = (
    (1, 0, ((2, 2),)), (-1, 1, ((2, 2),)),
    (1, 0, ((1, 1),)), (1, 1, ((1, 1),)), (-1, 0, ((1, 1),)), (-1, 1, ((1, 1),)),
)
CHAINS = {("y", "r"): Y_RING, ("y", "d"): Y_DIRECT, ("z", "r"): Z_RING, ("z", "t"): Z_TWO, ("z", "m"): Z_MID}
OFFSETS = (4, 3, -3, 2, -2, 1, -1, 0)
SLAB = {offset: r for r, offset in enumerate(OFFSETS)}
SLAB[-4] = 0


class Ring:
    def __init__(self, block, width, phase, axis, style, first_slot):
        self.block, self.width, self.phase, self.axis = block, width, phase, axis
        self.chains = CHAINS[axis, style]
        self.slots, at = {}, 0
        for c, (_, _, hops) in enumerate(self.chains):
            for i in range(len(hops)):
                self.slots[c, i] = at
                at += 1
        self.count, self.first_slot = at, first_slot

    def half_shape(self):
        if self.phase == 2:
            return (32, self.width)
        return (NZ // 2, 64, self.width) if self.axis == "y" else (NY // 2, 64, self.width)

    def half_bytes(self):
        size = 2
        for extent in self.half_shape():
            size *= extent
        return size

    def last(self, c):
        return self.slots[c, len(self.chains[c][2]) - 1]

    def ready(self, c):
        _, half, hops = self.chains[c]
        if self.axis == "y":
            return 3 if half == 0 else 7
        return SLAB[self.chains[c][0] * hops[0][0]]


def rings_of(k):
    rings, slot = {}, 0
    for b, (_, width, first, style) in enumerate(BLOCKS[k]):
        for phase, axis in ((1, first), (2, "z" if first == "y" else "y")):
            rings[b, phase] = Ring(b, width, phase, axis, "r" if phase == 1 else style, slot)
            slot += rings[b, phase].count
    return rings, slot


def schedule(rate=46.0e3, latency=(3.0, 2.6), hop=0.75, step=0.06, slab=0.37, depth=(100.0, 2.0)):
    tick = itertools.count()
    rings = [rings_of(k)[0] for k in (0, 1)]
    left = [{key: len(ring.chains) for key, ring in rings[k].items()} for k in (0, 1)]
    inbox, ready, order = [[], []], [{}, {}], [[], []]
    queues, backlog, free, now = {}, {}, [0.0, 0.0], 0.0
    aside = [list(ASIDE), list(ASIDE)]

    def offer(k, key, c, i):
        ring = rings[k][key]
        sign, _, hops = ring.chains[c]
        rank = (1, key[0], i - len(hops)) if key[1] == 1 else (0, i - len(hops), key[0], -hops[i][1])
        heapq.heappush(ready[k].setdefault((ring.axis, sign), []), (rank, next(tick), key, c, i))

    def issue(k):
        for link, waiting in ready[k].items():
            while waiting and backlog.get((link, k), 0.0) / rate < depth[k]:
                _, _, key, c, i = heapq.heappop(waiting)
                ring = rings[k][key]
                size = ring.half_bytes() * ring.chains[c][2][i][1]
                queues.setdefault(link, ([], []))[k].append([size, key, c, i])
                backlog[link, k] = backlog.get((link, k), 0.0) + size
                order[k].append((now, "send", key, c, i))

    def fill(k):
        while aside[k]:
            name, length, first = aside[k][0]
            coming = inbox[k][0][0] if inbox[k] else now + 1.0
            if free[k] < first or (coming - free[k] < 0.6 * length and free[k] < first + 4.0):
                return
            order[k].append((free[k], "aside", name, 0, 0))
            free[k] += length
            aside[k].pop(0)

    for k in (0, 1):
        for r in range(len(OFFSETS)):
            heapq.heappush(inbox[k], (slab * (r + 1), -1, "slab", r, 0, 0))
    while True:
        coming = [(max(inbox[k][0][0], free[k]), 0, k, None) for k in (0, 1) if inbox[k]]
        for link, pair in queues.items():
            busy_now = [k for k in (0, 1) if pair[k]]
            coming += [(now + pair[k][0][0] * len(busy_now) / (2 * rate), 1, k, link) for k in busy_now]
        if not coming:
            for k in (0, 1):
                order[k] += [(now, "aside", name, 0, 0) for name, _, _ in aside[k]]
            return order
        at, what, k, link = min(coming, key=lambda c: c[0])
        if at > now:
            for line, pair in queues.items():
                busy_now = [j for j in (0, 1) if pair[j]]
                for j in busy_now:
                    moved = (at - now) * 2 * rate / len(busy_now)
                    pair[j][0][0] -= moved
                    backlog[line, j] -= moved
            now = at
        if what == 1:
            over, key, c, i = queues[link][k].pop(0)
            backlog[link, k] -= max(over, 0.0)
            late = latency[k] + hop * (rings[k][key].chains[c][2][i][1] - 1)
            heapq.heappush(inbox[k], (max(now + late, slab * len(OFFSETS) + 0.01), next(tick), "take", key, c, i))
            continue
        _, _, kind, key, c, i = heapq.heappop(inbox[k])
        if kind == "slab":
            order[k].append((now, "slab", key, 0, 0))
            for b in range(len(BLOCKS[k])):
                ring = rings[k][b, 1]
                for c in range(len(ring.chains)):
                    if ring.ready(c) == key:
                        offer(k, (b, 1), c, 0)
            free[k] = now
        else:
            free[k] = now + step
            order[k].append((now, "take", key, c, i))
            if i + 1 < len(rings[k][key].chains[c][2]):
                offer(k, key, c, i + 1)
            else:
                left[k][key] -= 1
                if left[k][key] == 0 and key[1] == 1:
                    second = (key[0], 2)
                    for c in range(len(rings[k][second].chains)):
                        offer(k, second, c, 0)
        issue(k)
        if kind == "take" or key == len(OFFSETS) - 1:
            fill(k)


def kernel(tok_hbm, cot_hbm, wg_hbm, wu_hbm, wd_hbm,
           ig_out, gate_out, up_out, down_out,
           xb, wgu, wd, gub, hid, acc, own_ig, ig_part, ig_send0, ig_send, ig_recv0, ig_recv,
           xr1, xr2, *rest):
    blks, rbufs, fins, finr = [], [], [], []
    for k in (0, 1):
        nb = len(BLOCKS[k])
        keys = [(b, phase) for b in range(nb) for phase in (1, 2)]
        blks.append(rest[:nb])
        rbufs.append(dict(zip(keys, rest[nb : 3 * nb])))
        fins.append(rest[3 * nb : 4 * nb])
        finr.append(rest[4 * nb : 5 * nb])
        rest = rest[5 * nb :]
    (load_sem, ag_send, ag_recv, rel_send, rel_recv, igx_send, igx_recv,
     xrs_send, xrs_recv, ring_send, ring_recv, fin_send, fin_recv) = rest

    rep, x, core = lax.axis_index("rep"), lax.axis_index("fs"), lax.axis_index("tp")
    z, y = rep // NY, lax.rem(rep, NY)
    right = (rep, lax.rem(x + 1, 4), core)
    left = (rep, lax.rem(x + 3, 4), core)
    partner = (rep, x, 1 - core)
    y_of = {s: (z * NY + lax.rem(y + s + NY, NY), x, core) for s in (1, -1, 2)}
    y_of[-2] = y_of[2]
    z_of = {s: (lax.rem(z + s + NZ, NZ) * NY + y, x, core) for s in (1, -1, 2, -2)}

    def remote(src, dst, send_sem, recv_sem, to):
        return pltpu.make_async_remote_copy(src_ref=src, dst_ref=dst, send_sem=send_sem,
                                            recv_sem=recv_sem, device_id=to, device_id_type=MESH)

    cols = pl.ds(pl.multiple_of(core * 384, 128), 384)
    load_tok = pltpu.make_async_copy(tok_hbm, xb.at[0, 0], load_sem.at[0])
    load_cot = pltpu.make_async_copy(cot_hbm, xb.at[0, 1], load_sem.at[1])
    load_w = [
        pltpu.make_async_copy(wg_hbm.at[:, cols], wgu.at[:, pl.ds(0, 384)], load_sem.at[2]),
        pltpu.make_async_copy(wu_hbm.at[:, cols], wgu.at[:, pl.ds(384, 384)], load_sem.at[3]),
        pltpu.make_async_copy(wd_hbm.at[:, cols], wd, load_sem.at[4]),
    ]
    load_tok.start()
    load_cot.start()
    for copy in load_w:
        copy.start()

    barrier = pltpu.get_barrier_semaphore()
    others = (right, left, partner, y_of[1], y_of[-1], y_of[2], *z_of.values())
    for other in others:
        pl.semaphore_signal(barrier, inc=1, device_id=other, device_id_type=MESH)
    pl.semaphore_wait(barrier, len(others))
    load_tok.wait()
    load_cot.wait()

    def own_piece(k, side):
        piece = k if side == 0 else (k + 2) % 4
        return remote(xb.at[0, :, pl.ds(32 * piece, 32)], xb.at[2 + k, :, pl.ds(32 * side, 32)],
                      ag_send.at[side, k], ag_recv.at[side, k], right if side == 0 else left)

    def passed_on(k, side):
        return remote(xb.at[2 + k, :, pl.ds(32 * side, 32)], xb.at[6 + k, :, pl.ds(32 * side, 32)],
                      ag_send.at[side, 4 + k], ag_recv.at[side, 4 + k], right if side == 0 else left)

    def arrival(k, side):
        here = xb.at[2 + k, :, pl.ds(32 * side, 32)]
        return remote(here, here, ag_send.at[side, k], ag_recv.at[side, k],
                      right if side == 0 else left)

    def relay(k):
        return remote(xb.at[2 + k, :, pl.ds(0, 64)], xb.at[2 + k, :, pl.ds(64, 64)],
                      rel_send.at[k], rel_recv.at[k], partner)

    own_to_partner = remote(xb.at[0], xb.at[1], rel_send.at[6], rel_recv.at[6], partner)
    for k in range(4):
        for side in (0, 1):
            own_piece(k, side).start()
        if k == 0:
            own_to_partner.start()
    for copy in load_w:
        copy.wait()

    def forward(s):
        rows = pl.ds(pl.multiple_of(s * 128, 128), 128)
        gu = jnp.dot(xb[s, 0], wgu[...], preferred_element_type=F32)
        hg = jnp.dot(xb[s, 1], wd[...], preferred_element_type=F32)
        gate, up = gu[:, :384], gu[:, 384:]
        sig = jax.nn.sigmoid(gate)
        act = gate * sig
        gub[rows, pl.ds(0, 384)] = (hg * up * sig * (1.0 + gate * (1.0 - sig))).astype(BF16)
        gub[rows, pl.ds(384, 384)] = (hg * act).astype(BF16)
        hid[rows, :] = (act * up).astype(BF16)

    def input_slice(s, n, store):
        rows = pl.ds(pl.multiple_of(s * 128, 128), 128)
        d = pl.ds(pl.multiple_of(n * 512, 512), 512)
        part = lax.dot_general(gub[rows, :], wgu[d, :], (((1,), (1,)), ((), ())),
                               preferred_element_type=F32)
        store(d, part.astype(BF16))

    def input_part(s, store):
        def some(n, carry):
            input_slice(s, n, store)
            return carry

        lax.fori_loop(0, 4, some, 0)

    def store_own(d, part):
        own_ig[:, d] = part

    def store_partner(d, part):
        ig_send0[:, d] = part

    send_ig0 = remote(ig_send0, ig_recv0, igx_send.at[6], igx_recv.at[6], partner)

    def send_ig(k):
        return remote(ig_send.at[k], ig_recv.at[k], igx_send.at[k], igx_recv.at[k], partner)

    def store_step(k):
        def store(d, part):
            ig_part[k, :, d] = part[:64]
            ig_send[k, :, d] = part[64:]
        return store

    def step_part(s):
        input_part(s, store_step(s - 2))
        send_ig(s - 2).start()

    def late_slice(n):
        s = 6 + n // 4
        input_slice(s, n % 4, store_step(s - 2))
        if n % 4 == 3:
            send_ig(s - 2).start()

    forward(0)
    input_part(0, store_own)
    own_to_partner.wait_recv()
    forward(1)
    input_part(1, store_partner)
    send_ig0.start()

    def take(k):
        arrival(k, 0).wait_recv()
        arrival(k, 1).wait_recv()
        relay(k).start()

    def early(k, carry):
        take(k)

        @pl.when(k < 2)
        def _():
            passed_on(k, 0).start()
            passed_on(k, 1).start()

        relay(k).wait_recv()
        forward(k + 2)
        step_part(k + 2)
        return carry

    lax.fori_loop(0, 4, early, 0)

    across = (((0,), (0,)), ((), ()))

    def products(j, first, count):
        d = pl.ds(pl.multiple_of(j * 256, 256), 256)
        rows = pl.ds(first * 128, count * 128)
        tok = xb[pl.ds(first, count), 0, :, d].reshape(count * 128, 256)
        cot = xb[pl.ds(first, count), 1, :, d].reshape(count * 128, 256)
        return (lax.dot_general(tok, gub[rows, :], across, preferred_element_type=F32),
                lax.dot_general(cot, hid[rows, :], across, preferred_element_type=F32))

    def first_sums(j, carry):
        a, b = products(j, 0, 6)
        acc[j, :, pl.ds(0, 768)] = a
        acc[j, :, pl.ds(768, 384)] = b
        return carry

    lax.fori_loop(0, 2, first_sums, 0)
    take(4)
    lax.fori_loop(2, 5, first_sums, 0)
    relay(4).wait_recv()
    forward(6)
    take(5)
    lax.fori_loop(5, 8, first_sums, 0)
    relay(5).wait_recv()
    forward(7)

    def half_of(k, ring, offset, half):
        blk = blks[k][ring.block]
        if ring.axis == "y":
            there = lax.rem(y + offset + NY, NY)
            if ring.phase == 1:
                return blk.at[pl.ds(4 * half, 4), there]
            return blk.at[SLAB[0], there, pl.ds(32 * half, 32)]
        if ring.phase == 1:
            return blk.at[SLAB[offset], pl.ds(2 * half, 2)]
        return blk.at[SLAB[offset], y, pl.ds(32 * half, 32)]

    def hop(k, ring, c, i):
        sign, half, hops = ring.chains[c]
        slot = ring.slots[c, i]
        sem = ring.first_slot + slot
        return remote(half_of(k, ring, sign * hops[i][0], half),
                      rbufs[k][ring.block, ring.phase].at[slot], ring_send.at[sem], ring_recv.at[sem],
                      (y_of if ring.axis == "y" else z_of)[sign * hops[i][1]])

    def add_into(dst, src):
        shape = dst.shape
        if len(shape) == 2:
            dst[...] = (dst[...].astype(F32) + src[...].astype(F32)).astype(BF16)
        else:
            def one(i, carry):
                dst[i] = (dst[i].astype(F32) + src[i].astype(F32)).astype(BF16)
                return carry
            lax.fori_loop(0, shape[0], one, 0)

    def last_sums(k, r):
        j = lax.rem(z + OFFSETS[r] + NZ, NZ)
        a, b = products(j, 6, 2)
        a = (acc[j, :, pl.ds(0, 768)] + a).astype(BF16)
        b = (acc[j, :, pl.ds(768, 384)] + b).astype(BF16)
        for i, (col, width, _, _) in enumerate(BLOCKS[k]):
            piece = a[:, col : col + width] if col < 768 else b[:, col - 768 : col - 768 + width]
            blks[k][i][r] = piece.reshape(NY, 64, width)


    def xrs(stage, way):
        rows = pl.ds(32 * way, 32)
        which = {0: (4, 2), 1: (2, 2), 2: (0, 2)}[stage]
        dst = xr1.at[way] if stage == 0 else xr2.at[way, pl.ds(which[0], 2)]
        return remote(ig_part.at[pl.ds(which[0], 2), rows], dst, xrs_send.at[stage, way],
                      xrs_recv.at[stage, way], left if way == 0 else right)

    def merge_part(k, carry):
        send_ig(k).wait_recv()
        ig_part[k] = (ig_part[k].astype(F32) + ig_recv[k].astype(F32)).astype(BF16)
        return carry

    def x_begin():
        lax.fori_loop(2, 6, merge_part, 0)
        for stage in (0, 1):
            for way in (0, 1):
                xrs(stage, way).start()
        lax.fori_loop(0, 2, merge_part, 0)
        send_ig0.wait_recv()

    def x_middle():
        for way in (0, 1):
            xrs(0, way).wait_recv()
        for k in range(2):
            for way in (0, 1):
                rows = pl.ds(32 * way, 32)
                ig_part[k, rows, :] = (ig_part[k, rows, :].astype(F32)
                                       + xr1[way, k].astype(F32)).astype(BF16)
        for way in (0, 1):
            xrs(2, way).start()

    def x_end():
        for stage in (1, 2):
            for way in (0, 1):
                xrs(stage, way).wait_recv()
        for piece in range(4):
            rows = pl.ds(32 * piece, 32)
            total = own_ig[rows, :].astype(F32) + ig_recv0[rows, :].astype(F32)
            total = total + xr2[0, piece].astype(F32) + xr2[1, (piece + 2) % 4].astype(F32)
            ig_out[rows, :] = total.astype(BF16)

    scale = float(32768) ** -0.5

    def fin_copy(k, b):
        return remote(fins[k][b].at[pl.ds(32 * (1 - k), 32)], finr[k][b],
                      fin_send.at[b], fin_recv.at[b], partner)

    def finish_block(k, ring):
        b = ring.block
        for half in (0, 1):
            total = half_of(k, ring, 0, half)[...].astype(F32)
            for c, (_, h, _) in enumerate(ring.chains):
                if h == half:
                    total = total + rbufs[k][b, 2][ring.last(c)].astype(F32)
            fins[k][b][pl.ds(32 * half, 32), :] = total * scale
        fin_copy(k, b).start()

    def place_out(k, b, value):
        col, width, _, _ = BLOCKS[k][b]
        at = col
        while at < col + width:
            count = min(384 - at % 384, col + width - at)
            which, there = at // 384, k * 384 + at % 384
            (gate_out, up_out, down_out)[which][:, pl.ds(there, count)] = (
                value[:, at - col : at - col + count])
            at += count

    orders = schedule()

    def scatter(k):
        rings, _ = rings_of(k)
        left_of = {key: len(ring.chains) for key, ring in rings.items()}
        slices = iter(range(8))
        acts = {"part": lambda: late_slice(next(slices)), "begin": x_begin, "middle": x_middle, "end": x_end}
        for at, what, key, c, i in orders[k]:
            if what == "slab":
                last_sums(k, key)
                continue
            if what == "aside":
                acts[key]()
                continue
            ring = rings[key]
            if what == "send":
                hop(k, ring, c, i).start()
                continue
            sign, half, hops = ring.chains[c]
            hop(k, ring, c, i).wait_recv()
            if i + 1 < len(hops):
                add_into(half_of(k, ring, sign * hops[i + 1][0], half),
                         rbufs[k][key].at[ring.slots[c, i]])
            else:
                left_of[key] -= 1
                if key[1] == 1:
                    add_into(half_of(k, ring, 0, half), rbufs[k][key].at[ring.slots[c, i]])
                elif left_of[key] == 0:
                    finish_block(k, ring)
        for b in range(len(BLOCKS[k])):
            place_out(k, b, fins[k][b][pl.ds(32 * k, 32), :])
        for b in range(len(BLOCKS[1 - k])):
            fin_copy(1 - k, b).wait_recv()
            place_out(1 - k, b, finr[1 - k][b][...])

        for ring in rings.values():
            for c, i in ring.slots:
                hop(k, ring, c, i).wait_send()
        for b in range(len(BLOCKS[k])):
            fin_copy(k, b).wait_send()

    for k in (0, 1):
        pl.when(core == k)(lambda k=k: scatter(k))

    for k in range(4):
        for side in (0, 1):
            own_piece(k, side).wait_send()
    for k in range(2):
        for side in (0, 1):
            passed_on(k, side).wait_send()
    for k in range(6):
        relay(k).wait_send()
        send_ig(k).wait_send()
    own_to_partner.wait_send()
    send_ig0.wait_send()
    for stage in range(3):
        for way in (0, 1):
            xrs(stage, way).wait_send()


def write_out(a, b, c, d, out_a, out_b, out_c, out_d, sems):
    copies = [pltpu.make_async_copy(src, dst, sems.at[i])
              for i, (src, dst) in enumerate(((a, out_a), (b, out_b), (c, out_c), (d, out_d)))]
    for copy in copies:
        copy.start()
    for copy in copies:
        copy.wait()


def on_device(tokens, cotangent, gate_weight, up_weight, down_weight_t):
    rings = [rings_of(k)[0] for k in (0, 1)]
    slots = max(rings_of(k)[1] for k in (0, 1))
    most = max(len(blocks) for blocks in BLOCKS)
    anywhere = pl.BlockSpec(memory_space=pl.ANY)
    vmem = pl.BlockSpec(memory_space=pltpu.VMEM)
    dma = pltpu.SemaphoreType.DMA
    results = pl.pallas_call(
        kernel,
        out_shape=(
            pltpu.VMEM((128, 2048), BF16),
            pltpu.VMEM((32, 768), F32),
            pltpu.VMEM((32, 768), F32),
            pltpu.VMEM((32, 768), F32),
        ),
        in_specs=[anywhere] * 5,
        out_specs=[vmem] * 4,
        scratch_shapes=[
            pltpu.VMEM((8, 2, 128, 2048), BF16),
            pltpu.VMEM((2048, 768), BF16),
            pltpu.VMEM((2048, 384), BF16),
            pltpu.VMEM((1024, 768), BF16),
            pltpu.VMEM((1024, 384), BF16),
            pltpu.VMEM((8, 256, 1152), F32),
            pltpu.VMEM((128, 2048), BF16),
            pltpu.VMEM((6, 64, 2048), BF16),
            pltpu.VMEM((128, 2048), BF16),
            pltpu.VMEM((6, 64, 2048), BF16),
            pltpu.VMEM((128, 2048), BF16),
            pltpu.VMEM((6, 64, 2048), BF16),
            pltpu.VMEM((2, 2, 32, 2048), BF16),
            pltpu.VMEM((2, 4, 32, 2048), BF16),
        ]
        + [
            ref
            for k in (0, 1)
            for ref in (
                [pltpu.VMEM((NZ, NY, 64, width), BF16) for _, width, _, _ in BLOCKS[k]]
                + [
                    pltpu.VMEM((rings[k][b, phase].count, *rings[k][b, phase].half_shape()), BF16)
                    for b in range(len(BLOCKS[k]))
                    for phase in (1, 2)
                ]
                + [pltpu.VMEM((64, width), F32) for _, width, _, _ in BLOCKS[k]]
                + [pltpu.VMEM((32, width), F32) for _, width, _, _ in BLOCKS[k]]
            )
        ]
        + [
            dma((5,)), dma((2, 6)), dma((2, 6)), dma((7,)), dma((7,)), dma((7,)), dma((7,)),
            dma((3, 2)), dma((3, 2)), dma((slots,)), dma((slots,)),
            dma((most,)), dma((most,)),
        ],
        compiler_params=pltpu.CompilerParams(
            collective_id=0, has_side_effects=True, vmem_limit_bytes=VMEM_LIMIT
        ),
    )(tokens, cotangent, gate_weight, up_weight, down_weight_t)
    return pl.pallas_call(
        write_out,
        out_shape=tuple(jax.ShapeDtypeStruct(r.shape, r.dtype) for r in results),
        in_specs=[vmem] * 4,
        out_specs=[anywhere] * 4,
        scratch_shapes=[dma((4,))],
        compiler_params=pltpu.CompilerParams(vmem_limit_bytes=4 * 1024 * 1024),
    )(*results)


def solution(mesh):
    rows, tall = P(("rep", "fs", "tp"), None), P(("rep", "tp"), "fs")
    return jax.shard_map(
        on_device,
        mesh=mesh,
        in_specs=(rows, rows, P(None, "fs"), P(None, "fs"), P(None, "fs")),
        out_specs=(rows, tall, tall, tall),
        check_vma=False,
    )
```

```python
import heapq
import itertools

import jax
import jax.numpy as jnp
from jax import lax
from jax.experimental import pallas as pl
from jax.experimental.pallas import tpu as pltpu
from jax.sharding import PartitionSpec as P

MESH = pl.DeviceIdType.MESH
F32 = jnp.float32
BF16 = jnp.bfloat16
VMEM_LIMIT = 56 * 1024 * 1024

NY, NZ = 4, 8
X_BEGIN, X_MIDDLE, X_END = 6.0, 14.0, 26.0
ASIDE = tuple(("part", 0.42, 0.0) for _ in range(8)) + (("begin", 0.45, 8.5), ("middle", 0.15, 18.5), ("end", 0.3, 29.5))
BLOCKS = (
    (
        (0, 128, "y", "m"),
        (128, 128, "y", "m"),
        (256, 256, "z", "r"),
        (512, 256, "z", "d"),
        (768, 128, "y", "t"),
        (896, 128, "y", "t"),
        (1024, 128, "z", "d"),
    ),
    (
        (768, 128, "z", "r"),
        (896, 128, "y", "r"),
        (0, 256, "y", "r"),
        (1024, 128, "y", "t"),
        (256, 256, "y", "t"),
        (512, 256, "z", "r"),
    ),
)
Y_RING = ((1, 0, ((2, 1), (1, 1))), (-1, 1, ((2, 1), (1, 1))), (1, 1, ((1, 1),)), (-1, 0, ((1, 1),)))
Z_RING = (
    (1, 0, ((4, 1), (3, 1), (2, 1), (1, 1))), (-1, 1, ((4, 1), (3, 1), (2, 1), (1, 1))),
    (1, 1, ((3, 1), (2, 1), (1, 1))), (-1, 0, ((3, 1), (2, 1), (1, 1))),
)
Z_TWO = (
    (1, 0, ((4, 2), (2, 2))), (-1, 1, ((4, 2), (2, 2))),
    (1, 0, ((3, 2), (1, 1))), (1, 1, ((3, 2), (1, 1))),
    (-1, 0, ((3, 2), (1, 1))), (-1, 1, ((3, 2), (1, 1))),
    (1, 1, ((2, 2),)), (-1, 0, ((2, 2),)),
)
Z_MID = (
    (1, 0, ((4, 1), (3, 2), (1, 1))), (-1, 1, ((4, 1), (3, 2), (1, 1))),
    (1, 1, ((3, 2), (1, 1))), (-1, 0, ((3, 2), (1, 1))),
    (1, 0, ((2, 2),)), (1, 1, ((2, 2),)), (-1, 0, ((2, 2),)), (-1, 1, ((2, 2),)),
)
Y_DIRECT = (
    (1, 0, ((2, 2),)), (-1, 1, ((2, 2),)),
    (1, 0, ((1, 1),)), (1, 1, ((1, 1),)), (-1, 0, ((1, 1),)), (-1, 1, ((1, 1),)),
)
CHAINS = {("y", "r"): Y_RING, ("y", "d"): Y_DIRECT, ("z", "r"): Z_RING, ("z", "t"): Z_TWO, ("z", "m"): Z_MID}
OFFSETS = (4, 3, -3, 2, -2, 1, -1, 0)
SLAB = {offset: r for r, offset in enumerate(OFFSETS)}
SLAB[-4] = 0


class Ring:
    def __init__(self, block, width, phase, axis, style, first_slot):
        self.block, self.width, self.phase, self.axis = block, width, phase, axis
        self.chains = CHAINS[axis, style]
        self.slots, at = {}, 0
        for c, (_, _, hops) in enumerate(self.chains):
            for i in range(len(hops)):
                self.slots[c, i] = at
                at += 1
        self.count, self.first_slot = at, first_slot

    def half_shape(self):
        if self.phase == 2:
            return (32, self.width)
        return (NZ // 2, 64, self.width) if self.axis == "y" else (NY // 2, 64, self.width)

    def half_bytes(self):
        size = 2
        for extent in self.half_shape():
            size *= extent
        return size

    def last(self, c):
        return self.slots[c, len(self.chains[c][2]) - 1]

    def ready(self, c):
        _, half, hops = self.chains[c]
        if self.axis == "y":
            return 3 if half == 0 else 7
        return SLAB[self.chains[c][0] * hops[0][0]]


def rings_of(k):
    rings, slot = {}, 0
    for b, (_, width, first, style) in enumerate(BLOCKS[k]):
        for phase, axis in ((1, first), (2, "z" if first == "y" else "y")):
            rings[b, phase] = Ring(b, width, phase, axis, "r" if phase == 1 else style, slot)
            slot += rings[b, phase].count
    return rings, slot


def schedule(rate=46.0e3, latency=(3.0, 2.6), hop=0.75, step=0.06, slab=0.37, depth=(3.0, 2.0)):
    tick = itertools.count()
    rings = [rings_of(k)[0] for k in (0, 1)]
    left = [{key: len(ring.chains) for key, ring in rings[k].items()} for k in (0, 1)]
    inbox, ready, order = [[], []], [{}, {}], [[], []]
    queues, backlog, free, now = {}, {}, [0.0, 0.0], 0.0
    aside = [list(ASIDE), list(ASIDE)]

    def offer(k, key, c, i):
        ring = rings[k][key]
        sign, _, hops = ring.chains[c]
        rank = (1, key[0], i - len(hops)) if key[1] == 1 else (0, i - len(hops), key[0], -hops[i][1])
        heapq.heappush(ready[k].setdefault((ring.axis, sign), []), (rank, next(tick), key, c, i))

    def issue(k):
        for link, waiting in ready[k].items():
            while waiting and backlog.get((link, k), 0.0) / rate < depth[k]:
                _, _, key, c, i = heapq.heappop(waiting)
                ring = rings[k][key]
                size = ring.half_bytes() * ring.chains[c][2][i][1]
                queues.setdefault(link, ([], []))[k].append([size, key, c, i])
                backlog[link, k] = backlog.get((link, k), 0.0) + size
                order[k].append((now, "send", key, c, i))

    def fill(k):
        while aside[k]:
            name, length, first = aside[k][0]
            coming = inbox[k][0][0] if inbox[k] else now + 1.0
            if free[k] < first or (coming - free[k] < 0.6 * length and free[k] < first + 4.0):
                return
            order[k].append((free[k], "aside", name, 0, 0))
            free[k] += length
            aside[k].pop(0)

    for k in (0, 1):
        for r in range(len(OFFSETS)):
            heapq.heappush(inbox[k], (slab * (r + 1), -1, "slab", r, 0, 0))
    while True:
        coming = [(max(inbox[k][0][0], free[k]), 0, k, None) for k in (0, 1) if inbox[k]]
        for link, pair in queues.items():
            busy_now = [k for k in (0, 1) if pair[k]]
            coming += [(now + pair[k][0][0] * len(busy_now) / (2 * rate), 1, k, link) for k in busy_now]
        if not coming:
            for k in (0, 1):
                order[k] += [(now, "aside", name, 0, 0) for name, _, _ in aside[k]]
            return order
        at, what, k, link = min(coming, key=lambda c: c[0])
        if at > now:
            for line, pair in queues.items():
                busy_now = [j for j in (0, 1) if pair[j]]
                for j in busy_now:
                    moved = (at - now) * 2 * rate / len(busy_now)
                    pair[j][0][0] -= moved
                    backlog[line, j] -= moved
            now = at
        if what == 1:
            over, key, c, i = queues[link][k].pop(0)
            backlog[link, k] -= max(over, 0.0)
            late = latency[k] + hop * (rings[k][key].chains[c][2][i][1] - 1)
            heapq.heappush(inbox[k], (max(now + late, slab * len(OFFSETS) + 0.01), next(tick), "take", key, c, i))
            continue
        _, _, kind, key, c, i = heapq.heappop(inbox[k])
        if kind == "slab":
            order[k].append((now, "slab", key, 0, 0))
            for b in range(len(BLOCKS[k])):
                ring = rings[k][b, 1]
                for c in range(len(ring.chains)):
                    if ring.ready(c) == key:
                        offer(k, (b, 1), c, 0)
            free[k] = now
        else:
            free[k] = now + step
            order[k].append((now, "take", key, c, i))
            if i + 1 < len(rings[k][key].chains[c][2]):
                offer(k, key, c, i + 1)
            else:
                left[k][key] -= 1
                if left[k][key] == 0 and key[1] == 1:
                    second = (key[0], 2)
                    for c in range(len(rings[k][second].chains)):
                        offer(k, second, c, 0)
        issue(k)
        if kind == "take" or key == len(OFFSETS) - 1:
            fill(k)


def kernel(tok_hbm, cot_hbm, wg_hbm, wu_hbm, wd_hbm,
           ig_out, gate_out, up_out, down_out,
           xb, wgu, wd, gub, hid, acc, own_ig, ig_part, ig_send0, ig_send, ig_recv0, ig_recv,
           xr1, xr2, *rest):
    blks, rbufs, fins, finr = [], [], [], []
    for k in (0, 1):
        nb = len(BLOCKS[k])
        keys = [(b, phase) for b in range(nb) for phase in (1, 2)]
        blks.append(rest[:nb])
        rbufs.append(dict(zip(keys, rest[nb : 3 * nb])))
        fins.append(rest[3 * nb : 4 * nb])
        finr.append(rest[4 * nb : 5 * nb])
        rest = rest[5 * nb :]
    (load_sem, ag_send, ag_recv, rel_send, rel_recv, igx_send, igx_recv,
     xrs_send, xrs_recv, ring_send, ring_recv, fin_send, fin_recv) = rest

    rep, x, core = lax.axis_index("rep"), lax.axis_index("fs"), lax.axis_index("tp")
    z, y = rep // NY, lax.rem(rep, NY)
    right = (rep, lax.rem(x + 1, 4), core)
    left = (rep, lax.rem(x + 3, 4), core)
    partner = (rep, x, 1 - core)
    y_of = {s: (z * NY + lax.rem(y + s + NY, NY), x, core) for s in (1, -1, 2)}
    y_of[-2] = y_of[2]
    z_of = {s: (lax.rem(z + s + NZ, NZ) * NY + y, x, core) for s in (1, -1, 2, -2)}

    def remote(src, dst, send_sem, recv_sem, to):
        return pltpu.make_async_remote_copy(src_ref=src, dst_ref=dst, send_sem=send_sem,
                                            recv_sem=recv_sem, device_id=to, device_id_type=MESH)

    cols = pl.ds(pl.multiple_of(core * 384, 128), 384)
    load_tok = pltpu.make_async_copy(tok_hbm, xb.at[0, 0], load_sem.at[0])
    load_cot = pltpu.make_async_copy(cot_hbm, xb.at[0, 1], load_sem.at[1])
    load_w = [
        pltpu.make_async_copy(wg_hbm.at[:, cols], wgu.at[:, pl.ds(0, 384)], load_sem.at[2]),
        pltpu.make_async_copy(wu_hbm.at[:, cols], wgu.at[:, pl.ds(384, 384)], load_sem.at[3]),
        pltpu.make_async_copy(wd_hbm.at[:, cols], wd, load_sem.at[4]),
    ]
    load_tok.start()
    load_cot.start()
    for copy in load_w:
        copy.start()

    barrier = pltpu.get_barrier_semaphore()
    others = (right, left, partner, y_of[1], y_of[-1], y_of[2], *z_of.values())
    for other in others:
        pl.semaphore_signal(barrier, inc=1, device_id=other, device_id_type=MESH)
    pl.semaphore_wait(barrier, len(others))
    load_tok.wait()
    load_cot.wait()

    def own_piece(k, side):
        piece = k if side == 0 else (k + 2) % 4
        return remote(xb.at[0, :, pl.ds(32 * piece, 32)], xb.at[2 + k, :, pl.ds(32 * side, 32)],
                      ag_send.at[side, k], ag_recv.at[side, k], right if side == 0 else left)

    def passed_on(k, side):
        return remote(xb.at[2 + k, :, pl.ds(32 * side, 32)], xb.at[6 + k, :, pl.ds(32 * side, 32)],
                      ag_send.at[side, 4 + k], ag_recv.at[side, 4 + k], right if side == 0 else left)

    def arrival(k, side):
        here = xb.at[2 + k, :, pl.ds(32 * side, 32)]
        return remote(here, here, ag_send.at[side, k], ag_recv.at[side, k],
                      right if side == 0 else left)

    def relay(k):
        return remote(xb.at[2 + k, :, pl.ds(0, 64)], xb.at[2 + k, :, pl.ds(64, 64)],
                      rel_send.at[k], rel_recv.at[k], partner)

    own_to_partner = remote(xb.at[0], xb.at[1], rel_send.at[6], rel_recv.at[6], partner)
    for k in range(4):
        for side in (0, 1):
            own_piece(k, side).start()
        if k == 0:
            own_to_partner.start()
    for copy in load_w:
        copy.wait()

    def forward(s):
        rows = pl.ds(pl.multiple_of(s * 128, 128), 128)
        gu = jnp.dot(xb[s, 0], wgu[...], preferred_element_type=F32)
        hg = jnp.dot(xb[s, 1], wd[...], preferred_element_type=F32)
        gate, up = gu[:, :384], gu[:, 384:]
        sig = jax.nn.sigmoid(gate)
        act = gate * sig
        gub[rows, pl.ds(0, 384)] = (hg * up * sig * (1.0 + gate * (1.0 - sig))).astype(BF16)
        gub[rows, pl.ds(384, 384)] = (hg * act).astype(BF16)
        hid[rows, :] = (act * up).astype(BF16)

    def input_slice(s, n, store):
        rows = pl.ds(pl.multiple_of(s * 128, 128), 128)
        d = pl.ds(pl.multiple_of(n * 512, 512), 512)
        part = lax.dot_general(gub[rows, :], wgu[d, :], (((1,), (1,)), ((), ())),
                               preferred_element_type=F32)
        store(d, part.astype(BF16))

    def input_part(s, store):
        def some(n, carry):
            input_slice(s, n, store)
            return carry

        lax.fori_loop(0, 4, some, 0)

    def store_own(d, part):
        own_ig[:, d] = part

    def store_partner(d, part):
        ig_send0[:, d] = part

    send_ig0 = remote(ig_send0, ig_recv0, igx_send.at[6], igx_recv.at[6], partner)

    def send_ig(k):
        return remote(ig_send.at[k], ig_recv.at[k], igx_send.at[k], igx_recv.at[k], partner)

    def store_step(k):
        def store(d, part):
            ig_part[k, :, d] = part[:64]
            ig_send[k, :, d] = part[64:]
        return store

    def step_part(s):
        input_part(s, store_step(s - 2))
        send_ig(s - 2).start()

    def late_slice(n):
        s = 6 + n // 4
        input_slice(s, n % 4, store_step(s - 2))
        if n % 4 == 3:
            send_ig(s - 2).start()

    forward(0)
    input_part(0, store_own)
    own_to_partner.wait_recv()
    forward(1)
    input_part(1, store_partner)
    send_ig0.start()

    def take(k):
        arrival(k, 0).wait_recv()
        arrival(k, 1).wait_recv()
        relay(k).start()

    def early(k, carry):
        take(k)

        @pl.when(k < 2)
        def _():
            passed_on(k, 0).start()
            passed_on(k, 1).start()

        relay(k).wait_recv()
        forward(k + 2)
        step_part(k + 2)
        return carry

    lax.fori_loop(0, 4, early, 0)

    across = (((0,), (0,)), ((), ()))

    def products(j, first, count):
        d = pl.ds(pl.multiple_of(j * 256, 256), 256)
        rows = pl.ds(first * 128, count * 128)
        tok = xb[pl.ds(first, count), 0, :, d].reshape(count * 128, 256)
        cot = xb[pl.ds(first, count), 1, :, d].reshape(count * 128, 256)
        return (lax.dot_general(tok, gub[rows, :], across, preferred_element_type=F32),
                lax.dot_general(cot, hid[rows, :], across, preferred_element_type=F32))

    def first_sums(j, carry):
        a, b = products(j, 0, 6)
        acc[j, :, pl.ds(0, 768)] = a
        acc[j, :, pl.ds(768, 384)] = b
        return carry

    lax.fori_loop(0, 2, first_sums, 0)
    take(4)
    lax.fori_loop(2, 6, first_sums, 0)
    relay(4).wait_recv()
    forward(6)
    take(5)
    lax.fori_loop(6, 8, first_sums, 0)
    relay(5).wait_recv()
    forward(7)

    def half_of(k, ring, offset, half):
        blk = blks[k][ring.block]
        if ring.axis == "y":
            there = lax.rem(y + offset + NY, NY)
            if ring.phase == 1:
                return blk.at[pl.ds(4 * half, 4), there]
            return blk.at[SLAB[0], there, pl.ds(32 * half, 32)]
        if ring.phase == 1:
            return blk.at[SLAB[offset], pl.ds(2 * half, 2)]
        return blk.at[SLAB[offset], y, pl.ds(32 * half, 32)]

    def hop(k, ring, c, i):
        sign, half, hops = ring.chains[c]
        slot = ring.slots[c, i]
        sem = ring.first_slot + slot
        return remote(half_of(k, ring, sign * hops[i][0], half),
                      rbufs[k][ring.block, ring.phase].at[slot], ring_send.at[sem], ring_recv.at[sem],
                      (y_of if ring.axis == "y" else z_of)[sign * hops[i][1]])

    def add_into(dst, src):
        shape = dst.shape
        if len(shape) == 2:
            dst[...] = (dst[...].astype(F32) + src[...].astype(F32)).astype(BF16)
        else:
            def one(i, carry):
                dst[i] = (dst[i].astype(F32) + src[i].astype(F32)).astype(BF16)
                return carry
            lax.fori_loop(0, shape[0], one, 0)

    def last_sums(k, r):
        j = lax.rem(z + OFFSETS[r] + NZ, NZ)
        a, b = products(j, 6, 2)
        a = (acc[j, :, pl.ds(0, 768)] + a).astype(BF16)
        b = (acc[j, :, pl.ds(768, 384)] + b).astype(BF16)
        for i, (col, width, _, _) in enumerate(BLOCKS[k]):
            piece = a[:, col : col + width] if col < 768 else b[:, col - 768 : col - 768 + width]
            blks[k][i][r] = piece.reshape(NY, 64, width)


    def xrs(stage, way):
        rows = pl.ds(32 * way, 32)
        which = {0: (4, 2), 1: (2, 2), 2: (0, 2)}[stage]
        dst = xr1.at[way] if stage == 0 else xr2.at[way, pl.ds(which[0], 2)]
        return remote(ig_part.at[pl.ds(which[0], 2), rows], dst, xrs_send.at[stage, way],
                      xrs_recv.at[stage, way], left if way == 0 else right)

    def merge_part(k, carry):
        send_ig(k).wait_recv()
        ig_part[k] = (ig_part[k].astype(F32) + ig_recv[k].astype(F32)).astype(BF16)
        return carry

    def x_begin():
        lax.fori_loop(2, 6, merge_part, 0)
        for stage in (0, 1):
            for way in (0, 1):
                xrs(stage, way).start()
        lax.fori_loop(0, 2, merge_part, 0)
        send_ig0.wait_recv()

    def x_middle():
        for way in (0, 1):
            xrs(0, way).wait_recv()
        for k in range(2):
            for way in (0, 1):
                rows = pl.ds(32 * way, 32)
                ig_part[k, rows, :] = (ig_part[k, rows, :].astype(F32)
                                       + xr1[way, k].astype(F32)).astype(BF16)
        for way in (0, 1):
            xrs(2, way).start()

    def x_end():
        for stage in (1, 2):
            for way in (0, 1):
                xrs(stage, way).wait_recv()
        for piece in range(4):
            rows = pl.ds(32 * piece, 32)
            total = own_ig[rows, :].astype(F32) + ig_recv0[rows, :].astype(F32)
            total = total + xr2[0, piece].astype(F32) + xr2[1, (piece + 2) % 4].astype(F32)
            ig_out[rows, :] = total.astype(BF16)

    scale = float(32768) ** -0.5

    def fin_copy(k, b):
        return remote(fins[k][b].at[pl.ds(32 * (1 - k), 32)], finr[k][b],
                      fin_send.at[b], fin_recv.at[b], partner)

    def finish_block(k, ring):
        b = ring.block
        for half in (0, 1):
            total = half_of(k, ring, 0, half)[...].astype(F32)
            for c, (_, h, _) in enumerate(ring.chains):
                if h == half:
                    total = total + rbufs[k][b, 2][ring.last(c)].astype(F32)
            fins[k][b][pl.ds(32 * half, 32), :] = total * scale
        fin_copy(k, b).start()

    def place_out(k, b, value):
        col, width, _, _ = BLOCKS[k][b]
        at = col
        while at < col + width:
            count = min(384 - at % 384, col + width - at)
            which, there = at // 384, k * 384 + at % 384
            (gate_out, up_out, down_out)[which][:, pl.ds(there, count)] = (
                value[:, at - col : at - col + count])
            at += count

    orders = schedule()

    def scatter(k):
        rings, _ = rings_of(k)
        left_of = {key: len(ring.chains) for key, ring in rings.items()}
        slices = iter(range(8))
        acts = {"part": lambda: late_slice(next(slices)), "begin": x_begin, "middle": x_middle, "end": x_end}
        for at, what, key, c, i in orders[k]:
            if what == "slab":
                last_sums(k, key)
                continue
            if what == "aside":
                acts[key]()
                continue
            ring = rings[key]
            if what == "send":
                hop(k, ring, c, i).start()
                continue
            sign, half, hops = ring.chains[c]
            hop(k, ring, c, i).wait_recv()
            if i + 1 < len(hops):
                add_into(half_of(k, ring, sign * hops[i + 1][0], half),
                         rbufs[k][key].at[ring.slots[c, i]])
            else:
                left_of[key] -= 1
                if key[1] == 1:
                    add_into(half_of(k, ring, 0, half), rbufs[k][key].at[ring.slots[c, i]])
                elif left_of[key] == 0:
                    finish_block(k, ring)
        for b in range(len(BLOCKS[k])):
            place_out(k, b, fins[k][b][pl.ds(32 * k, 32), :])
        for b in range(len(BLOCKS[1 - k])):
            fin_copy(1 - k, b).wait_recv()
            place_out(1 - k, b, finr[1 - k][b][...])

        for ring in rings.values():
            for c, i in ring.slots:
                hop(k, ring, c, i).wait_send()
        for b in range(len(BLOCKS[k])):
            fin_copy(k, b).wait_send()

    for k in (0, 1):
        pl.when(core == k)(lambda k=k: scatter(k))

    for k in range(4):
        for side in (0, 1):
            own_piece(k, side).wait_send()
    for k in range(2):
        for side in (0, 1):
            passed_on(k, side).wait_send()
    for k in range(6):
        relay(k).wait_send()
        send_ig(k).wait_send()
    own_to_partner.wait_send()
    send_ig0.wait_send()
    for stage in range(3):
        for way in (0, 1):
            xrs(stage, way).wait_send()


def write_out(a, b, c, d, out_a, out_b, out_c, out_d, sems):
    copies = [pltpu.make_async_copy(src, dst, sems.at[i])
              for i, (src, dst) in enumerate(((a, out_a), (b, out_b), (c, out_c), (d, out_d)))]
    for copy in copies:
        copy.start()
    for copy in copies:
        copy.wait()


def on_device(tokens, cotangent, gate_weight, up_weight, down_weight_t):
    rings = [rings_of(k)[0] for k in (0, 1)]
    slots = max(rings_of(k)[1] for k in (0, 1))
    most = max(len(blocks) for blocks in BLOCKS)
    anywhere = pl.BlockSpec(memory_space=pl.ANY)
    vmem = pl.BlockSpec(memory_space=pltpu.VMEM)
    dma = pltpu.SemaphoreType.DMA
    results = pl.pallas_call(
        kernel,
        out_shape=(
            pltpu.VMEM((128, 2048), BF16),
            pltpu.VMEM((32, 768), F32),
            pltpu.VMEM((32, 768), F32),
            pltpu.VMEM((32, 768), F32),
        ),
        in_specs=[anywhere] * 5,
        out_specs=[vmem] * 4,
        scratch_shapes=[
            pltpu.VMEM((8, 2, 128, 2048), BF16),
            pltpu.VMEM((2048, 768), BF16),
            pltpu.VMEM((2048, 384), BF16),
            pltpu.VMEM((1024, 768), BF16),
            pltpu.VMEM((1024, 384), BF16),
            pltpu.VMEM((8, 256, 1152), F32),
            pltpu.VMEM((128, 2048), BF16),
            pltpu.VMEM((6, 64, 2048), BF16),
            pltpu.VMEM((128, 2048), BF16),
            pltpu.VMEM((6, 64, 2048), BF16),
            pltpu.VMEM((128, 2048), BF16),
            pltpu.VMEM((6, 64, 2048), BF16),
            pltpu.VMEM((2, 2, 32, 2048), BF16),
            pltpu.VMEM((2, 4, 32, 2048), BF16),
        ]
        + [
            ref
            for k in (0, 1)
            for ref in (
                [pltpu.VMEM((NZ, NY, 64, width), BF16) for _, width, _, _ in BLOCKS[k]]
                + [
                    pltpu.VMEM((rings[k][b, phase].count, *rings[k][b, phase].half_shape()), BF16)
                    for b in range(len(BLOCKS[k]))
                    for phase in (1, 2)
                ]
                + [pltpu.VMEM((64, width), F32) for _, width, _, _ in BLOCKS[k]]
                + [pltpu.VMEM((32, width), F32) for _, width, _, _ in BLOCKS[k]]
            )
        ]
        + [
            dma((5,)), dma((2, 6)), dma((2, 6)), dma((7,)), dma((7,)), dma((7,)), dma((7,)),
            dma((3, 2)), dma((3, 2)), dma((slots,)), dma((slots,)),
            dma((most,)), dma((most,)),
        ],
        compiler_params=pltpu.CompilerParams(
            collective_id=0, has_side_effects=True, vmem_limit_bytes=VMEM_LIMIT
        ),
    )(tokens, cotangent, gate_weight, up_weight, down_weight_t)
    return pl.pallas_call(
        write_out,
        out_shape=tuple(jax.ShapeDtypeStruct(r.shape, r.dtype) for r in results),
        in_specs=[vmem] * 4,
        out_specs=[anywhere] * 4,
        scratch_shapes=[dma((4,))],
        compiler_params=pltpu.CompilerParams(vmem_limit_bytes=4 * 1024 * 1024),
    )(*results)


def solution(mesh):
    rows, tall = P(("rep", "fs", "tp"), None), P(("rep", "tp"), "fs")
    return jax.shard_map(
        on_device,
        mesh=mesh,
        in_specs=(rows, rows, P(None, "fs"), P(None, "fs"), P(None, "fs")),
        out_specs=(rows, tall, tall, tall),
        check_vma=False,
    )
```
